32 devices in a mesh: sp: 8 (over z, y), dp: 4 (over x, core).
Axes of the slice: x: 2, y: 2, z: 4, core: 2. Of those that a mesh axis runs over, the one named last changes fastest.
Arguments:
- tokens: bfloat16 [4, 2048, 2048], P('dp', 'sp'), may hold values from -6 to 6
- in_gain: float32 [2048], replicated, may hold values from 0.1 to 1.9
- w_query_down: bfloat16 [2048, 512], P('dp'), may hold values from -0.125 to 0.125
- w_latent_down: bfloat16 [2048, 256], P('dp'), may hold values from -0.125 to 0.125
- w_rope_key: bfloat16 [2048, 64], replicated, may hold values from -0.125 to 0.125
- query_latent_gain: float32 [512], replicated, may hold values from 0.1 to 1.9
- latent_gain: float32 [256], replicated, may hold values from 0.1 to 1.9
- w_query_up: bfloat16 [512, 3072], P('dp', 'sp'), may hold values from -0.25 to 0.25
- w_key_up: bfloat16 [256, 2048], P('dp', 'sp'), may hold values from -0.375 to 0.375
- w_value_up: bfloat16 [256, 2048], P('dp', 'sp'), may hold values from -0.375 to 0.375
- query_gain: float32 [192], replicated, may hold values from 0.5 to 14
- key_gain: float32 [192], replicated, may hold values from 0.5 to 14
- out_gain: float32 [2048], replicated, may hold values from 0.1 to 1.9
- w_out: bfloat16 [2048, 2048], P(('sp', 'dp')), may hold values from -0.125 to 0.125
Outputs:
- result: bfloat16 [4, 2048, 2048], P('dp', 'sp')
The draws below stay inside these ranges and needn't reach their ends.
All inputs are finite; a program needn't handle non-finite values.
Results may differ from the reference program's by a relative error of at most 0.034.
The reference program's roundings to bfloat16 on the way count: a program that leaves them out, or rounds other values in their place, can miss the bound.
Values may be sent and summed in bfloat16 or wider, within the bound.
A program may use at most 64 MiB of HBM per device.

```python
import jax
import jax.numpy as jnp
from jax import lax

D = 2048
HEADS = 16
NOPE = 128
ROPE = 64
VD = 128
QR = 512
KR = 256
QK = 192
LEN = 2048
SEQS = 4


def gain_vector(key, member):
    spread = jnp.clip(jax.random.normal(jax.random.fold_in(key, 11 + member), (QK,), jnp.float32), -2.5, 2.5)
    return (1.0 + 0.18 * spread).astype(jnp.float32)


def draw_query_gain(key, part):
    return gain_vector(key, 0)


def draw_key_gain(key, part):
    return gain_vector(key, 1)


def block_levels(own_key, shape, split, least, largest):
    gain, own = 1.0, jax.random.fold_in(own_key, 6)
    for dim, parts in split:
        draws = jnp.exp(jax.random.uniform(jax.random.fold_in(own, dim), (parts,), jnp.float32, least / len(split), largest / len(split)))
        gain = gain * jnp.repeat(draws, shape[dim] // parts).reshape([-1 if axis == dim else 1 for axis in range(len(shape))])
    return gain


def centred(stream_key, shape, scale, limit, split=(), kind=jnp.bfloat16):
    values = jax.random.normal(stream_key, shape, jnp.float32) * scale
    if len(split) > 0:
        values = block_levels(stream_key, shape, split, -0.22, 0.18) * values
    return jnp.clip(values, min=-limit, max=limit).astype(kind)


def setup_inputs(seed: int = 0) -> dict:
    arg_keys = jax.random.split(jax.random.key(seed), 15)
    tokens = centred(arg_keys[0], (SEQS, LEN, D), 1.0, 6.0, ((0, 4), (1, 8)))
    in_gain = jnp.clip(1.0 + 0.18 * jax.random.normal(arg_keys[1], (D,), jnp.float32), 0.1, 1.9)
    w_query_down = centred(arg_keys[2], (D, QR), D ** -0.5, 0.125, ((0, 4),))
    w_latent_down = centred(arg_keys[3], (D, KR), D ** -0.5, 0.125, ((0, 4),))
    w_rope_key = centred(arg_keys[4], (D, ROPE), D ** -0.5, 0.125)
    query_latent_gain = jnp.clip(1.0 + 0.18 * jax.random.normal(arg_keys[5], (QR,), jnp.float32), 0.1, 1.9)
    latent_gain = jnp.clip(1.0 + 0.18 * jax.random.normal(arg_keys[6], (KR,), jnp.float32), 0.1, 1.9)
    w_query_up = centred(arg_keys[7], (QR, HEADS * QK), QR ** -0.5, 0.25, ((0, 4), (1, 8)))
    w_key_up = centred(arg_keys[8], (KR, HEADS * NOPE), KR ** -0.5, 0.375, ((0, 4), (1, 8)))
    w_value_up = centred(arg_keys[9], (KR, HEADS * VD), KR ** -0.5, 0.375, ((0, 4), (1, 8)))
    query_gain = draw_query_gain(jax.random.fold_in(arg_keys[14], 71), 0)
    key_gain = draw_key_gain(jax.random.fold_in(arg_keys[14], 71), 0)
    out_gain = jnp.clip(1.0 + 0.18 * jax.random.normal(arg_keys[12], (HEADS * VD,), jnp.float32), 0.1, 1.9)
    w_out = centred(arg_keys[13], (HEADS * VD, D), (HEADS * VD) ** -0.5, 0.125, ((0, 32),))
    return dict(tokens=tokens, in_gain=in_gain, w_query_down=w_query_down, w_latent_down=w_latent_down, w_rope_key=w_rope_key, query_latent_gain=query_latent_gain, latent_gain=latent_gain, w_query_up=w_query_up, w_key_up=w_key_up, w_value_up=w_value_up, query_gain=query_gain, key_gain=key_gain, out_gain=out_gain, w_out=w_out)


EPS = 1e-06
THETA = 10000.0
NEG_BIG = -1e+30

def rms_scale(values, scaling):
    return values * lax.rsqrt(lax.optimization_barrier(jnp.mean(values * values, axis=-1, keepdims=True)) + EPS) * scaling

def rotate(tail_part, positions):
    half_width = tail_part.shape[-1] // 2
    frequency = THETA ** (-jnp.arange(half_width, dtype=jnp.float32) / half_width)
    angles = positions[:, None] * frequency[None, :]
    cosine = jnp.cos(angles)[:, None, :]
    sine = jnp.sin(angles)[:, None, :]
    first_half = tail_part[..., :half_width]
    second_half = tail_part[..., half_width:]
    return jnp.concatenate([first_half * cosine - second_half * sine, second_half * cosine + first_half * sine], axis=-1)

def finish_heads(joined, positions, scaling, rope_width):
    row_count = joined.shape[0]
    normal = rms_scale(joined, scaling)
    turned = rotate(normal[..., -rope_width:], positions)
    return jnp.concatenate([normal[..., :-rope_width], turned], axis=-1).astype(jnp.bfloat16).reshape(row_count, -1)

def attend(queries, keys, values, head_count):
    length = queries.shape[0]
    block_rows = min(512, length)
    query_blocks = queries.reshape(length // block_rows, block_rows, head_count, -1)
    key_heads = keys.reshape(length, head_count, -1).astype(jnp.float32)
    value_heads = values.reshape(length, head_count, -1).astype(jnp.float32)
    score_scale = key_heads.shape[-1] ** (-0.5)
    key_pos = jnp.arange(length)

    def one_block(block_args):
        query_block, block_index = block_args
        scores = jnp.einsum('qhd,khd->hqk', query_block.astype(jnp.float32), key_heads) * score_scale
        query_pos = block_index * block_rows + jnp.arange(block_rows)
        allowed = key_pos[None, :] <= query_pos[:, None]
        scores = jnp.where(allowed[None], scores, NEG_BIG)
        weights = jax.nn.softmax(scores, axis=-1).astype(jnp.bfloat16)
        return jnp.einsum('hqk,khd->qhd', weights.astype(jnp.float32), value_heads).astype(jnp.bfloat16)
    outcome = lax.map(one_block, (query_blocks, jnp.arange(length // block_rows)))
    return outcome.reshape(length, -1)

def reference(tokens, in_gain, w_query_down, w_latent_down, w_rope_key, query_latent_gain, latent_gain, w_query_up, w_key_up, w_value_up, query_gain, key_gain, out_gain, w_out):

    def one_sequence(sequence):
        normed = rms_scale(sequence.astype(jnp.float32), in_gain).astype(jnp.bfloat16)
        latent_q = rms_scale(jnp.dot(normed, w_query_down, preferred_element_type=jnp.float32), query_latent_gain).astype(jnp.bfloat16)
        latent_kv = rms_scale(jnp.dot(normed, w_latent_down, preferred_element_type=jnp.float32), latent_gain).astype(jnp.bfloat16)
        rope_key = jnp.dot(normed, w_rope_key, preferred_element_type=jnp.float32).astype(jnp.bfloat16)
        positions = jnp.arange(LEN, dtype=jnp.float32)
        query_total = jnp.dot(latent_q, w_query_up, preferred_element_type=jnp.float32)
        queries = finish_heads(query_total.reshape(LEN, HEADS, QK), positions, query_gain, ROPE)
        key_total = jnp.dot(latent_kv, w_key_up, preferred_element_type=jnp.float32).reshape(LEN, HEADS, NOPE)
        shared = jnp.broadcast_to(rope_key.astype(jnp.float32)[:, None, :], (LEN, HEADS, ROPE))
        keys = finish_heads(jnp.concatenate([key_total, shared], axis=-1), positions, key_gain, ROPE)
        values = jnp.dot(latent_kv, w_value_up, preferred_element_type=jnp.float32).astype(jnp.bfloat16)
        attended = attend(queries, keys, values, HEADS)
        mixed = rms_scale(attended.astype(jnp.float32), out_gain).astype(jnp.bfloat16)
        return jnp.dot(mixed, w_out, preferred_element_type=jnp.float32).astype(jnp.bfloat16)
    return lax.map(one_sequence, tokens)
```

```python
import functools

import jax
import jax.numpy as jnp
import numpy as np
from jax import lax
from jax.experimental import pallas as pl
from jax.experimental.pallas import tpu as pltpu
from jax.sharding import PartitionSpec as P

HEADS = 16
EPS = 1e-06
THETA = 10000.0
NEG_BIG = -1e30
LOG2E = 1.4426950408889634
NT = (((1,), (1,)), ((), ()))


def rms_scale(values, scaling):
    return values * lax.rsqrt(jnp.mean(values * values, axis=-1, keepdims=True) + EPS) * scaling


def swap_halves(x):
    half = x.shape[-1] // 2
    return jnp.concatenate([x[..., half:], x[..., :half]], axis=-1)


def rotation_table(length, width):
    half = width // 2
    frequency = np.float32(THETA) ** (-np.arange(half, dtype=np.float32) / np.float32(half))
    angles = np.arange(length, dtype=np.float32)[:, None] * frequency[None, :]
    cosine, sine = np.cos(angles), np.sin(angles)
    return np.concatenate([cosine, cosine, -sine, sine], axis=-1).astype(np.float32)


def with_swapped(x):
    return jnp.concatenate([x, swap_halves(x)], axis=-1)


def head_finish(t1, t2, r, gain, turn):
    rope2 = t2.shape[1]
    y = t2 * r * turn
    return (t1 * r * gain).astype(jnp.bfloat16), y + pltpu.roll(y, rope2 // 2, 1)


def project_queries(rows, heads, nope, lq, wq, gain, turn, q_s):
    wide = wq.shape[1] // heads
    rope2 = wide - nope
    inv = 1.0 / (nope + rope2 // 2)
    q = jnp.dot(lq, wq[...], preferred_element_type=jnp.float32)
    for h in range(heads):
        t1 = q[:, h * wide : h * wide + nope]
        t2 = q[:, h * wide + nope : (h + 1) * wide]
        r = lax.rsqrt(jnp.sum(t1 * t1 + 0.5 * t2 * t2, axis=-1, keepdims=True) * inv + EPS)
        first, last = head_finish(t1, t2, r, gain, turn)
        q_s[h, :, 0:nope] = first
        q_s[h, :, nope:wide] = last.astype(jnp.bfloat16)


def pack_rope(rope_key):
    part = rope_key.shape[0] // 4
    band = [rope_key[g * part : (g + 1) * part] for g in range(4)]
    return jnp.concatenate(band, axis=1).astype(jnp.bfloat16)


def unpack_rope(packed, rope2):
    quarter = rope2 // 4
    lane = lax.broadcasted_iota(jnp.int32, (packed.shape[0], rope2), 1)
    bands = []
    for g in range(4):
        p = packed[:, (g // 2) * rope2 : (g // 2 + 1) * rope2].astype(jnp.float32)
        if g % 2 == 0:
            front, b, a = p, pltpu.roll(p, quarter, 1), pltpu.roll(p, 3 * quarter, 1)
        else:
            front, b, a = pltpu.roll(p, 2 * quarter, 1), pltpu.roll(p, 3 * quarter, 1), pltpu.roll(p, quarter, 1)
        bands.append(jnp.where(lane < 2 * quarter, front, jnp.where(lane < 3 * quarter, b, a)))
    return jnp.concatenate(bands, axis=0)


def project_keys(block, rows, nope, lkv, shared, wks, wvt, gain, turn, k_s, v_s):
    tok = pl.ds(pl.multiple_of(block * rows, rows), rows)
    rope2 = shared.shape[1]
    wide = nope + rope2
    inv = 1.0 / (nope + rope2 // 2)
    v_s[:, tok] = lax.dot_general(wvt[...], lkv, NT, preferred_element_type=jnp.float32).astype(jnp.bfloat16)
    half_sq = 0.5 * shared * shared
    lane = lax.broadcasted_iota(jnp.int32, (rows, rope2), 1)
    turned = shared * turn
    turned = turned + pltpu.roll(turned, rope2 // 2, 1)
    turned = jnp.where(lane < rope2 // 2, turned, 0.0)
    h = 0
    for wk in wks:
        k = jnp.dot(lkv, wk, preferred_element_type=jnp.float32)
        for j in range(k.shape[1] // nope):
            t1 = k[:, j * nope : (j + 1) * nope]
            r = lax.rsqrt(jnp.sum(t1 * t1 + half_sq, axis=-1, keepdims=True) * inv + EPS)
            k_s[h, tok, 0:nope] = (t1 * r * gain).astype(jnp.bfloat16)
            k_s[h, tok, nope:wide] = (turned * r).astype(jnp.bfloat16)
            h += 1


def attend_block(qb, rows, chunk, heads, vd, scale, q_s, k_s, v_s):
    qs = [q_s[h] for h in range(heads)]
    factor = scale * LOG2E

    def step(kb, carry, masked):
        ktok = pl.ds(pl.multiple_of(kb * chunk, chunk), chunk)
        new = []
        for h in range(heads):
            m, l, acc = carry[h]
            s = lax.dot_general(k_s[h, ktok, :], qs[h], NT, preferred_element_type=jnp.float32) * factor
            if masked:
                kpos = kb * chunk + lax.broadcasted_iota(jnp.int32, (chunk, rows), 0)
                qpos = qb * rows + lax.broadcasted_iota(jnp.int32, (chunk, rows), 1)
                s = jnp.where(kpos <= qpos, s, NEG_BIG)
            m_new = jnp.maximum(m, jnp.max(s, axis=0, keepdims=True))
            alpha = jnp.exp2(m - m_new)
            p = jnp.exp2(s - m_new)
            l = l * alpha + jnp.sum(p, axis=0, keepdims=True)
            vt = v_s[h * vd : (h + 1) * vd, ktok]
            acc = acc * alpha + jnp.dot(vt, p.astype(jnp.bfloat16), preferred_element_type=jnp.float32)
            new.append((m_new, l, acc))
        return tuple(new)

    carry = tuple(
        (
            jnp.full((1, rows), NEG_BIG, jnp.float32),
            jnp.zeros((1, rows), jnp.float32),
            jnp.zeros((vd, rows), jnp.float32),
        )
        for _ in range(heads)
    )
    last = (qb * rows) // chunk
    carry = lax.fori_loop(0, last, lambda kb, c: step(kb, c, False), carry)
    carry = step(last, carry, True)
    return jnp.concatenate([jnp.transpose(acc / l) for _, l, acc in carry], axis=1).astype(jnp.bfloat16)


MESH = pl.DeviceIdType.MESH


class Links:
    def __init__(self, send_sems, recv_sems, send_rows, recv_rows):
        self.send_sems, self.recv_sems, self.ids, self.sent = send_sems, recv_sems, {}, []
        self.send_rows, self.recv_rows, self.row_ids = send_rows, recv_rows, {}

    def sems(self, role, at):
        if at is None:
            n = self.ids.setdefault(role, len(self.ids))
            return self.send_sems.at[n], self.recv_sems.at[n]
        n = self.row_ids.setdefault(role, len(self.row_ids))
        return self.send_rows.at[n, at], self.recv_rows.at[n, at]

    def copy(self, role, at, src, dst, target, land=None):
        send, recv = self.sems(role, at)
        if land is not None:
            recv = self.sems(role, land)[1]
        return pltpu.make_async_remote_copy(
            src_ref=src, dst_ref=dst, send_sem=send, recv_sem=recv, device_id=target, device_id_type=MESH,
        )

    def send(self, role, src, dst, target, ok=None, at=None):
        self.sent.append((ok, role, at, src, dst, target))
        guard(ok, lambda: self.copy(role, at, src, dst, target).start())

    def arrive(self, role, dst, target, ok=None, at=None):
        guard(ok, lambda: self.copy(role, at, dst, dst, target).wait_recv())

    def drain(self):
        for ok, role, at, src, dst, target in self.sent:
            guard(ok, lambda: self.copy(role, at, src, dst, target).wait_send())
        self.sent = []


def guard(ok, action):
    if ok is None:
        action()
    else:
        pl.when(ok)(action)


DOWN_CUTS = (1, 2)


def sem_counts(nx, ny, nz, cores):
    items = sum(DOWN_CUTS)
    over, pair = nx - 1, cores - 1
    down = items * over * ny * (1 + pair) + 2 * pair
    up = 3 * (over + (ny - 1) + over * (ny - 1) + nx * ny * pair)
    rows = 2 + (ny - 1) + 2 + 1 + 2 + (ny - 1) + ny * over + ny * nx * pair
    return down + up, rows


def layer_kernel(
    dims, chunk, heads, nope, vd, scale,
    tokens, in_gain, wqd, wld, wrope, q_lat_gain, kv_lat_gain, wqu, wku, wvu, q_gain, k_gain, table, out_gain, w_out,
    out,
    normed, wqd_g, wld_g, wqu_g, wku_g, wvu_g, w_g, wq_s, wvt, kv_g, q_g, q_s, k_s, v_s, att_s, heads_g,
    send_sems, recv_sems, send_rows, recv_rows,
):
    nx, ny, nz, cores = dims
    seqs, dps = ny * nz, nx * cores
    rows = tokens.shape[0]
    s, d = lax.axis_index("sp"), lax.axis_index("dp")
    y, z = lax.rem(s, ny), lax.div(s, ny)
    c, x = lax.rem(d, cores), lax.div(d, cores)
    links = Links(send_sems, recv_sems, send_rows, recv_rows)

    def at_sp(target):
        return {"sp": target, "dp": d}

    def at_dp(target):
        return {"sp": s, "dp": target}

    def at_z(target):
        return at_sp(target * ny + y)

    def at_y(step):
        return at_sp(z * ny + lax.rem(y + step, ny))

    def at_x(step):
        return at_dp(lax.rem(x + step, nx) * cores + c)

    def at_core(step):
        return at_dp(x * cores + lax.rem(c + step, cores))

    def back_y(step):
        return lax.rem(y - step + ny, ny)

    def back_x(step):
        return lax.rem(x - step + nx, nx)

    def back_core(step):
        return lax.rem(c - step + cores, cores)

    barrier = pltpu.get_barrier_semaphore()
    peers = [at_z(lax.rem(z + k, nz)) for k in range(1, nz)] + [at_y(k) for k in range(1, ny)]
    peers += [at_x(k) for k in range(1, nx)] + [at_core(k) for k in range(1, cores)]
    for peer in peers:
        pl.semaphore_signal(barrier, inc=1, device_id=peer, device_id_type=MESH)
    pl.semaphore_wait(barrier, len(peers))

    xs, ys, cs = range(1, nx), range(1, ny), range(1, cores)

    downs = ((wld, wld_g, DOWN_CUTS[0]), (wqd, wqd_g, DOWN_CUTS[1]))
    items = [(a, cut) for a in range(2) for cut in range(downs[a][2])]

    def piece(ref, a, cut, which):
        cuts = downs[a][2]
        part = ref.shape[0] // (ny * cuts)
        return ref.at[pl.ds(pl.multiple_of((which * cuts + cut) * part, part), part)]

    for it, (a, cut) in enumerate(items):
        src, dst, _ = downs[a]
        for dx in xs:
            links.send(("x", it, dx), piece(src, a, cut, y), piece(dst.at[d], a, cut, y), at_x(dx))
    for a, (src, dst, _) in enumerate(downs):
        for dc in cs:
            links.send(("c", a, dc), src, dst.at[d], at_core(dc))

    ups = ((wqu, wqu_g), (wku, wku_g), (wvu, wvu_g))
    for a, (src, dst) in enumerate(ups):
        for dy in ys:
            links.send(("uy", a, dy), src, dst.at[y, d], at_y(dy))
        for dx in xs:
            links.send(("ux", a, dx), src, dst.at[y, d], at_x(dx))
        for dc in cs:
            links.send(("uc", a, 0, 0, dc), src, dst.at[y, d], at_core(dc))

    part_out = w_out.shape[0]

    def w_block(zz, yy, xx, cc):
        first = ((zz * ny + yy) * dps + xx * cores + cc) * part_out
        return w_g.at[pl.ds(pl.multiple_of(first, part_out), part_out)]

    def along_z(role, way, origin, src, dst, ok):
        links.send((role, way), src, dst, at_z(jnp.clip(z + way, 0, nz - 1)), ok, at=origin)

    def z_arrival(step, way):
        origin = z - way * (step + 1)
        ok = (origin >= 0) & (origin < nz)
        return jnp.clip(origin, 0, nz - 1), ok, ok & (z + way >= 0) & (z + way < nz)

    def w_over_y(origin, src, ok):
        for dy in ys:
            links.send(("wy", dy), src, w_block(origin, y, x, c), at_y(dy), ok, at=origin)

    def w_over_x(origin, dyo, src, ok):
        for dx in xs:
            links.send(("wx", dyo, dx), src, w_block(origin, back_y(dyo), x, c), at_x(dx), ok, at=origin)

    def w_over_core(origin, dyo, dxo, src, ok):
        for dc in cs:
            dst = w_block(origin, back_y(dyo), back_x(dxo), c)
            links.send(("wc", dyo, dxo, dc), src, dst, at_core(dc), ok, at=origin)

    def w_z_arrive(step):
        for way in (1, -1):
            origin, ok, _ = z_arrival(step, way)
            block = w_block(origin, y, x, c)
            links.arrive(("wz", way), block, at_sp(s), ok, at=origin)
            w_over_x(origin, 0, block, ok)
            w_over_core(origin, 0, 0, block, ok)

    def w_z_relay(step):
        for way in (1, -1):
            origin, _, more = z_arrival(step, way)
            block = w_block(origin, y, x, c)
            along_z("wz", way, origin, block, block, more)

    def w_y_send(step):
        for way in (1, -1):
            origin, ok, _ = z_arrival(step, way)
            w_over_y(origin, w_block(origin, y, x, c), ok)

    def w_y_arrive_at(origin, ok):
        for dy in ys:
            block = w_block(origin, back_y(dy), x, c)
            links.arrive(("wy", dy), block, at_sp(s), ok, at=origin)
            w_over_x(origin, dy, block, ok)
            w_over_core(origin, dy, 0, block, ok)

    def w_y_arrive(step):
        for way in (1, -1):
            origin, ok, _ = z_arrival(step, way)
            w_y_arrive_at(origin, ok)

    def w_x_arrive(origin, dyo):
        for dx in xs:
            block = w_block(origin, back_y(dyo), back_x(dx), c)
            links.arrive(("wx", dyo, dx), block, at_dp(d), at=origin)
            w_over_core(origin, dyo, dx, block, None)

    own_block = w_block(z, y, x, c)
    for way in (1, -1):
        if nz > 1:
            along_z("wz", way, z, w_out, own_block, (z + way >= 0) & (z + way < nz))
    w_over_x(z, 0, w_out, None)
    w_over_core(z, 0, 0, w_out, None)

    for src, dst, _ in downs:
        dst[d] = src[...]
    for src, dst in ups:
        dst[y, d] = src[...]
    own_out = pl.ds(pl.multiple_of((s * dps + d) * part_out, part_out), part_out)
    w_g[own_out, :] = w_out[...]

    def norm(i, _):
        step = rows // 4
        band = pl.ds(pl.multiple_of(i * step, step), step)
        normed[band, :] = rms_scale(tokens[band, :].astype(jnp.float32), in_gain[...]).astype(jnp.bfloat16)
        return 0

    lax.fori_loop(0, 4, norm, 0)
    rope_key = lax.dot_general(normed[...], wrope[...], NT, preferred_element_type=jnp.float32)
    kv_g[s, rows:, :] = pack_rope(rope_key)

    def down_x(it):
        a, cut = items[it]
        dst = downs[a][1]
        for dx in xs:
            got = piece(dst.at[back_x(dx) * cores + c], a, cut, y)
            links.arrive(("x", it, dx), got, at_dp(d))
            for dy in ys:
                links.send(("y", it, dx, dy), got, got, at_y(dy))
            for dc in cs:
                links.send(("cx", it, dx, dc), got, got, at_core(dc))

    def down_y(it):
        a, cut = items[it]
        dst = downs[a][1]
        for dx in xs:
            for dy in ys:
                got = piece(dst.at[back_x(dx) * cores + c], a, cut, back_y(dy))
                links.arrive(("y", it, dx, dy), got, at_dp(d))
                for dc in cs:
                    links.send(("cy", it, dx, dy, dc), got, got, at_core(dc))

    def settle_down(a):
        dst = downs[a][1]
        for dc in cs:
            links.arrive(("c", a, dc), dst.at[x * cores + back_core(dc)], at_dp(d))
            for it in range(len(items)):
                if items[it][0] != a:
                    continue
                for dx in xs:
                    origin = dst.at[back_x(dx) * cores + back_core(dc)]
                    links.arrive(("cx", it, dx, dc), piece(origin, a, items[it][1], y), at_dp(d))
                    for dy in ys:
                        got = piece(origin, a, items[it][1], back_y(dy))
                        links.arrive(("cy", it, dx, dy, dc), got, at_dp(d))

    def down(gathered):
        part = gathered.shape[1]
        total = None
        for k in range(dps):
            term = jnp.dot(normed[:, k * part : (k + 1) * part], gathered[k], preferred_element_type=jnp.float32)
            total = term if total is None else total + term
        return total

    def kv_over_y(zz, ok=None):
        block = kv_g.at[zz * ny + y]
        for dy in ys:
            links.send(("kvy", dy), block, block, at_y(dy), ok, at=zz)

    def launch(role, block):
        for way in (1, -1):
            if nz > 1:
                along_z(role, way, z, block, block, (z + way >= 0) & (z + way < nz))

    down_x(0)
    down_x(1)
    down_y(0)
    if nz > 1:
        w_z_arrive(0)
        w_z_relay(0)
    for it in range(2, len(items)):
        down_x(it)
    settle_down(0)
    kv_g[s, :rows, :] = rms_scale(down(wld_g), kv_lat_gain[...]).astype(jnp.bfloat16)
    launch("kv", kv_g.at[s])
    kv_over_y(z)
    for it in range(1, len(items)):
        down_y(it)

    def up_spread(a):
        dst = ups[a][1]
        for dy in ys:
            got = dst.at[back_y(dy), d]
            links.arrive(("uy", a, dy), got, at_dp(d))
            for dc in cs:
                links.send(("uc", a, dy, 0, dc), got, got, at_core(dc))
        for dx in xs:
            got = dst.at[y, back_x(dx) * cores + c]
            links.arrive(("ux", a, dx), got, at_dp(d))
            for dy in ys:
                links.send(("uxy", a, dx, dy), got, got, at_y(dy))
            for dc in cs:
                links.send(("uc", a, 0, dx, dc), got, got, at_core(dc))

    def up_diagonal(a):
        dst = ups[a][1]
        for dx in xs:
            for dy in ys:
                got = dst.at[back_y(dy), back_x(dx) * cores + c]
                links.arrive(("uxy", a, dx, dy), got, at_dp(d))
                for dc in cs:
                    links.send(("uc", a, dy, dx, dc), got, got, at_core(dc))

    def settle_up(a):
        dst = ups[a][1]
        for dy in range(ny):
            for dx in range(nx):
                for dc in cs:
                    got = dst.at[back_y(dy), back_x(dx) * cores + back_core(dc)]
                    links.arrive(("uc", a, dy, dx, dc), got, at_dp(d))

    settle_down(1)
    q_g[z] = rms_scale(down(wqd_g), q_lat_gain[...]).astype(jnp.bfloat16)
    launch("q", q_g.at[z])

    def z_relay(role, step, buffer, after=None):
        for way in (1, -1):
            origin, ok, more = z_arrival(step, way)
            block = buffer(origin)
            links.arrive((role, way), block, at_sp(s), ok, at=origin)
            along_z(role, way, origin, block, block, more)
            if after is not None:
                after(origin, ok)

    def kv_block(zz):
        return kv_g.at[zz * ny + y]

    for a in range(3):
        up_spread(a)
    if nz > 1:
        z_relay("kv", 0, kv_block, kv_over_y)
    for a in range(3):
        up_diagonal(a)
    for a in range(3):
        settle_up(a)
    shard_heads = heads // ny
    depth = wqu.shape[0]
    for yy in range(ny):
        for k in range(dps):
            up = wqu_g[yy, k].astype(jnp.float32)
            width = wqu.shape[1] // shard_heads
            for h in range(shard_heads):
                head = up[:, h * width : (h + 1) * width]
                both = jnp.concatenate([head[:, :nope], with_swapped(head[:, nope:])], axis=1)
                wide = both.shape[1]
                first = (yy * shard_heads + h) * wide
                wq_s[k * depth : (k + 1) * depth, first : first + wide] = both.astype(jnp.bfloat16)
        wv = wvu_g[yy].reshape(dps * wvu.shape[0], wvu.shape[1])
        wvt[yy * shard_heads * vd : (yy + 1) * shard_heads * vd, :] = jnp.transpose(
            wv.astype(jnp.float32)
        ).astype(jnp.bfloat16)
    gq, gk = q_gain[:, :nope], k_gain[:, :nope]
    gq2, gk2 = with_swapped(q_gain[:, nope:]), with_swapped(k_gain[:, nope:])
    rope2 = gq2.shape[1]

    def project_kv(block):
        tok = pl.ds(pl.multiple_of(block * rows, rows), rows)
        wks = [wku_g[yy].reshape(dps * wku.shape[0], wku.shape[1]) for yy in range(ny)]
        shared = unpack_rope(kv_g[block, rows:, :], rope2)
        project_keys(block, rows, nope, kv_g[block, :rows, :], shared, wks, wvt, gk, table[tok, :] * gk2, k_s, v_s)

    def near(i):
        m = jnp.minimum(z, nz - 1 - z)
        two = i <= 2 * m
        dist = jnp.where(two, lax.div(i + 1, 2), i - m)
        up = jnp.where(two, lax.rem(i, 2) == 1, z < nz - 1 - z)
        return jnp.where(up, z + dist, z - dist)

    def kv_column(zz):
        def one(j, _):
            yy = lax.rem(y + j, ny)
            project_kv(zz * ny + yy)
            return 0

        for dy in ys:
            links.arrive(("kvy", dy), kv_g.at[zz * ny + back_y(dy)], at_sp(s), at=zz)
        lax.fori_loop(0, ny, one, 0)

    def kv_columns(first, last):
        def one(i, _):
            kv_column(near(i))
            return 0

        lax.fori_loop(first, last, one, 0)

    kv_columns(0, 1)
    for step in range(1, nz - 1):
        z_relay("kv", step, kv_block, kv_over_y)
        if step < nz - 2:
            w_z_arrive(step)
        z_relay("q", step - 1, lambda zz: q_g.at[zz])
    for step in range(1, nz - 2):
        w_z_relay(step)
    w_over_y(z, w_out, None)
    for step in range(nz - 1):
        if step < nz - 2:
            w_y_send(step)
    kv_columns(1, nz)
    if nz > 1:
        z_relay("q", nz - 2, lambda zz: q_g.at[zz])

    def hand_over(zz):
        return links.copy("a2a", zz, att_s.at[zz], heads_g.at[z], at_z(zz), land=z)

    def attend(i, _):
        zz = near(lax.rem(i + 1, nz))
        qb = zz * ny + y
        tok = pl.ds(pl.multiple_of(qb * rows, rows), rows)
        project_queries(rows, heads, nope, q_g[zz], wq_s, gq, table[tok, :] * gq2, q_s)
        att_s[zz] = attend_block(qb, rows, chunk, heads, vd, scale, q_s, k_s, v_s)

        @pl.when(i < nz - 1)
        def _():
            hand_over(zz).start()

        return 0

    def attend_range(first, last):
        lax.fori_loop(first, last, attend, 0)

    cuts = [(k * nz) // 4 for k in range(5)]
    attend_range(cuts[0], cuts[1])
    w_y_arrive_at(z, None)
    attend_range(cuts[1], cuts[2])
    if nz > 1:
        w_y_arrive(0)
        w_z_arrive(nz - 2) if nz > 2 else None
        w_y_send(nz - 2)
    attend_range(cuts[2], cuts[3])
    for step in range(1, nz - 2):
        w_y_arrive(step)
    for k in range(nz):
        w_x_arrive(lax.rem(z + k, nz), 0)
    attend_range(cuts[3], cuts[4])
    if nz > 1:
        for step in range(max(nz - 2, 1), nz - 1):
            w_y_arrive(step)
    for k in range(nz):
        for dy in ys:
            w_x_arrive(lax.rem(z + k, nz), dy)
    heads_g[z] = att_s[z]
    for k in range(1, nz):
        origin = lax.rem(z + k, nz)
        links.copy("a2a", origin, att_s.at[origin], heads_g.at[z], at_z(origin), land=origin).wait_send()
        links.copy("a2a", origin, heads_g.at[origin], heads_g.at[origin], at_z(origin), land=origin).wait_recv()
    width = heads * vd
    square = jnp.zeros((rows, 1), jnp.float32)
    for k in range(nz):
        block = heads_g[k].astype(jnp.float32)
        square = square + jnp.sum(block * block, axis=-1, keepdims=True)
    r = lax.rsqrt(square * (1.0 / (nz * width)) + EPS)
    for k in range(nz):
        cols = slice(k * width, (k + 1) * width)
        normed[:, cols] = (heads_g[k].astype(jnp.float32) * r * out_gain[:, cols]).astype(jnp.bfloat16)
    for k in range(nz):
        origin = lax.rem(z + k, nz)
        for dy in range(ny):
            for dx in range(nx):
                for dc in cs:
                    block = w_block(origin, back_y(dy), back_x(dx), back_core(dc))
                    links.arrive(("wc", dy, dx, dc), block, at_dp(d), at=origin)
    tile = 256 if out.shape[1] % 256 == 0 else out.shape[1]

    def project_out(i, _):
        cols = pl.ds(pl.multiple_of(i * tile, tile), tile)
        out[:, cols] = jnp.dot(normed[...], w_g[:, cols], preferred_element_type=jnp.float32).astype(out.dtype)
        return 0

    lax.fori_loop(0, out.shape[1] // tile, project_out, 0)
    links.drain()


def per_device(
    tokens, in_gain, w_query_down, w_latent_down, w_rope_key, query_latent_gain, latent_gain,
    w_query_up, w_key_up, w_value_up, query_gain, key_gain, out_gain, w_out,
):
    seqs, dps = lax.axis_size("sp"), lax.axis_size("dp")
    cores = 2 if dps % 2 == 0 else 1
    nx = dps // cores
    ny = nx if seqs % nx == 0 else 1
    nz = seqs // ny
    heads = HEADS // nz
    own_rows = tokens.shape[1]
    length = own_rows * seqs
    rope = w_rope_key.shape[1]
    nope = w_key_up.shape[1] * ny // heads
    vd = w_value_up.shape[1] * ny // heads
    wide = nope + 2 * rope
    chunk = min(2 * own_rows, length)
    sems, sem_rows = sem_counts(nx, ny, nz, cores)
    b16 = jnp.bfloat16

    def gathered(w, *lead):
        return pltpu.VMEM(lead + (dps,) + w.shape, b16)

    result = pl.pallas_call(
        functools.partial(
            layer_kernel, (nx, ny, nz, cores), chunk, heads, nope, vd, float(nope + rope) ** -0.5
        ),
        out_shape=jax.ShapeDtypeStruct((own_rows, w_out.shape[1]), b16),
        in_specs=[pl.BlockSpec(memory_space=pltpu.VMEM)] * 15,
        out_specs=pl.BlockSpec(memory_space=pltpu.VMEM),
        scratch_shapes=[
            pltpu.VMEM((own_rows, max(tokens.shape[2], w_out.shape[0] * seqs * dps)), b16),
            gathered(w_query_down), gathered(w_latent_down),
            gathered(w_query_up, ny), gathered(w_key_up, ny), gathered(w_value_up, ny),
            pltpu.VMEM((w_out.shape[0] * seqs * dps, w_out.shape[1]), b16),
            pltpu.VMEM((w_query_down.shape[1], heads * wide), b16),
            pltpu.VMEM((heads * vd, w_latent_down.shape[1]), b16),
            pltpu.VMEM((seqs, own_rows + own_rows * rope // w_latent_down.shape[1], w_latent_down.shape[1]), b16),
            pltpu.VMEM((nz, own_rows, w_query_down.shape[1]), b16),
            pltpu.VMEM((heads, own_rows, wide), b16),
            pltpu.VMEM((heads, length, wide), b16),
            pltpu.VMEM((heads * vd, length), b16),
            pltpu.VMEM((nz, own_rows, heads * vd), b16),
            pltpu.VMEM((nz, own_rows, heads * vd), b16),
            pltpu.SemaphoreType.DMA((sems,)),
            pltpu.SemaphoreType.DMA((sems,)),
            pltpu.SemaphoreType.DMA((sem_rows, nz)),
            pltpu.SemaphoreType.DMA((sem_rows, nz)),
        ],
        compiler_params=pltpu.CompilerParams(
            vmem_limit_bytes=56 * 1024 * 1024, collective_id=0, has_side_effects=True
        ),
        cost_estimate=pl.CostEstimate(flops=60 * 10**9, bytes_accessed=10**8, transcendentals=5 * 10**6),
    )(
        tokens.reshape(own_rows, tokens.shape[2]), in_gain[None], w_query_down, w_latent_down, w_rope_key.T,
        query_latent_gain[None], latent_gain[None], w_query_up, w_key_up, w_value_up,
        query_gain[None], key_gain[None], jnp.asarray(rotation_table(length, rope)), out_gain[None], w_out,
    )
    return result.reshape(1, own_rows, w_out.shape[1])


def solution(mesh):
    in_specs = (
        P("dp", "sp", None), P(), P("dp", None), P("dp", None), P(), P(), P(),
        P("dp", "sp"), P("dp", "sp"), P("dp", "sp"), P(), P(), P(), P(("sp", "dp"), None),
    )
    return jax.shard_map(
        per_device, mesh=mesh, in_specs=in_specs, out_specs=P("dp", "sp", None), check_vma=False
    )
```

```python
import functools

import jax
import jax.numpy as jnp
import numpy as np
from jax import lax
from jax.experimental import pallas as pl
from jax.experimental.pallas import tpu as pltpu
from jax.sharding import PartitionSpec as P

HEADS = 16
EPS = 1e-06
THETA = 10000.0
NEG_BIG = -1e30
LOG2E = 1.4426950408889634
NT = (((1,), (1,)), ((), ()))


def rms_scale(values, scaling):
    return values * lax.rsqrt(jnp.mean(values * values, axis=-1, keepdims=True) + EPS) * scaling


def swap_halves(x):
    half = x.shape[-1] // 2
    return jnp.concatenate([x[..., half:], x[..., :half]], axis=-1)


def rotation_table(length, width):
    half = width // 2
    frequency = np.float32(THETA) ** (-np.arange(half, dtype=np.float32) / np.float32(half))
    angles = np.arange(length, dtype=np.float32)[:, None] * frequency[None, :]
    cosine, sine = np.cos(angles), np.sin(angles)
    return np.concatenate([cosine, cosine, -sine, sine], axis=-1).astype(np.float32)


def with_swapped(x):
    return jnp.concatenate([x, swap_halves(x)], axis=-1)


def head_finish(t1, t2, r, gain, turn):
    rope2 = t2.shape[1]
    y = t2 * r * turn
    return (t1 * r * gain).astype(jnp.bfloat16), y + pltpu.roll(y, rope2 // 2, 1)


def project_queries(rows, heads, nope, lq, wq, gain, turn, q_s):
    wide = wq.shape[1] // heads
    rope2 = wide - nope
    inv = 1.0 / (nope + rope2 // 2)
    q = jnp.dot(lq, wq[...], preferred_element_type=jnp.float32)
    for h in range(heads):
        t1 = q[:, h * wide : h * wide + nope]
        t2 = q[:, h * wide + nope : (h + 1) * wide]
        r = lax.rsqrt(jnp.sum(t1 * t1 + 0.5 * t2 * t2, axis=-1, keepdims=True) * inv + EPS)
        first, last = head_finish(t1, t2, r, gain, turn)
        q_s[h, :, 0:nope] = first
        q_s[h, :, nope:wide] = last.astype(jnp.bfloat16)


def pack_rope(rope_key):
    part = rope_key.shape[0] // 4
    band = [rope_key[g * part : (g + 1) * part] for g in range(4)]
    return jnp.concatenate(band, axis=1).astype(jnp.bfloat16)


def unpack_rope(packed, rope2):
    quarter = rope2 // 4
    lane = lax.broadcasted_iota(jnp.int32, (packed.shape[0], rope2), 1)
    bands = []
    for g in range(4):
        p = packed[:, (g // 2) * rope2 : (g // 2 + 1) * rope2].astype(jnp.float32)
        if g % 2 == 0:
            front, b, a = p, pltpu.roll(p, quarter, 1), pltpu.roll(p, 3 * quarter, 1)
        else:
            front, b, a = pltpu.roll(p, 2 * quarter, 1), pltpu.roll(p, 3 * quarter, 1), pltpu.roll(p, quarter, 1)
        bands.append(jnp.where(lane < 2 * quarter, front, jnp.where(lane < 3 * quarter, b, a)))
    return jnp.concatenate(bands, axis=0)


def project_keys(block, rows, nope, lkv, shared, wks, wvt, gain, turn, k_s, v_s):
    tok = pl.ds(pl.multiple_of(block * rows, rows), rows)
    rope2 = shared.shape[1]
    wide = nope + rope2
    inv = 1.0 / (nope + rope2 // 2)
    v_s[:, tok] = lax.dot_general(wvt[...], lkv, NT, preferred_element_type=jnp.float32).astype(jnp.bfloat16)
    half_sq = 0.5 * shared * shared
    lane = lax.broadcasted_iota(jnp.int32, (rows, rope2), 1)
    turned = shared * turn
    turned = turned + pltpu.roll(turned, rope2 // 2, 1)
    turned = jnp.where(lane < rope2 // 2, turned, 0.0)
    h = 0
    for wk in wks:
        k = jnp.dot(lkv, wk, preferred_element_type=jnp.float32)
        for j in range(k.shape[1] // nope):
            t1 = k[:, j * nope : (j + 1) * nope]
            r = lax.rsqrt(jnp.sum(t1 * t1 + half_sq, axis=-1, keepdims=True) * inv + EPS)
            k_s[h, tok, 0:nope] = (t1 * r * gain).astype(jnp.bfloat16)
            k_s[h, tok, nope:wide] = (turned * r).astype(jnp.bfloat16)
            h += 1


def attend_item(j, y, rows, chunk, heads, vd, scale, masked, q_s, k_s, v_s, m_s, l_s, acc_s, scores):
    ktok = pl.ds(pl.multiple_of(j * chunk, chunk), chunk)
    factor = scale * LOG2E
    sub = 128

    def product(h):
        scores[h] = lax.dot_general(k_s[h, ktok, :], q_s[h], NT, preferred_element_type=jnp.float32)

    def band(h, first):
        s = scores[h, first : first + sub, :]
        if masked:
            kpos = first + lax.broadcasted_iota(jnp.int32, (sub, rows), 0)
            qpos = y * rows + lax.broadcasted_iota(jnp.int32, (sub, rows), 1)
            s = jnp.where(kpos <= qpos, s, NEG_BIG)
        return s

    product(0)
    for h in range(heads):
        if h + 1 < heads:
            product(h + 1)
        top = None
        for first in range(0, chunk, sub):
            part = jnp.max(band(h, first).reshape(sub // 8, 8, rows), axis=0)
            top = part if top is None else jnp.maximum(top, part)
        m = m_s[h]
        m_new = jnp.maximum(m, jnp.max(top, axis=0, keepdims=True) * factor)
        alpha = jnp.exp2(m - m_new)
        total, weights = None, []
        for first in range(0, chunk, sub):
            p = jnp.exp2(band(h, first) * factor - m_new)
            part = jnp.sum(p.reshape(sub // 8, 8, rows), axis=0)
            total = part if total is None else total + part
            weights.append(p.astype(jnp.bfloat16))
        m_s[h] = m_new
        l_s[h] = l_s[h] * alpha + jnp.sum(total, axis=0, keepdims=True)
        vt = v_s[h * vd : (h + 1) * vd, ktok]
        acc_s[h] = acc_s[h] * alpha + jnp.dot(
            vt, jnp.concatenate(weights, axis=0), preferred_element_type=jnp.float32
        )


def attend_block(i, y, rows, chunk, heads, vd, scale, q_s, k_s, v_s, m_s, l_s, acc_s, scores):
    m_s[...] = jnp.full(m_s.shape, NEG_BIG, jnp.float32)
    l_s[...] = jnp.zeros(l_s.shape, jnp.float32)
    acc_s[...] = jnp.zeros(acc_s.shape, jnp.float32)

    def item(j, masked):
        attend_item(j, y, rows, chunk, heads, vd, scale, masked, q_s, k_s, v_s, m_s, l_s, acc_s, scores)

    def step(j, _):
        item(j, False)
        return 0

    lax.fori_loop(0, i, step, 0)
    item(i, True)
    return jnp.concatenate([jnp.transpose(acc_s[h] / l_s[h]) for h in range(heads)], axis=1).astype(jnp.bfloat16)


MESH = pl.DeviceIdType.MESH


class Links:
    def __init__(self, send_sems, recv_sems, send_rows, recv_rows):
        self.send_sems, self.recv_sems, self.ids, self.sent = send_sems, recv_sems, {}, []
        self.send_rows, self.recv_rows, self.row_ids = send_rows, recv_rows, {}

    def sems(self, role, at):
        if at is None:
            n = self.ids.setdefault(role, len(self.ids))
            return self.send_sems.at[n], self.recv_sems.at[n]
        n = self.row_ids.setdefault(role, len(self.row_ids))
        return self.send_rows.at[n, at], self.recv_rows.at[n, at]

    def copy(self, role, at, src, dst, target, land=None):
        send, recv = self.sems(role, at)
        if land is not None:
            recv = self.sems(role, land)[1]
        return pltpu.make_async_remote_copy(
            src_ref=src, dst_ref=dst, send_sem=send, recv_sem=recv, device_id=target, device_id_type=MESH,
        )

    def send(self, role, src, dst, target, ok=None, at=None):
        self.sent.append((ok, role, at, src, dst, target))
        guard(ok, lambda: self.copy(role, at, src, dst, target).start())

    def arrive(self, role, dst, target, ok=None, at=None):
        guard(ok, lambda: self.copy(role, at, dst, dst, target).wait_recv())

    def drain(self):
        for ok, role, at, src, dst, target in self.sent:
            guard(ok, lambda: self.copy(role, at, src, dst, target).wait_send())
        self.sent = []


def guard(ok, action):
    if ok is None:
        action()
    else:
        pl.when(ok)(action)


DOWN_CUTS = (1, 2)


def sem_counts(nx, ny, nz, cores):
    items = sum(DOWN_CUTS)
    over, pair = nx - 1, cores - 1
    down = items * over * ny * (1 + pair) + 2 * pair
    up = 3 * (over * ny + (ny - 1) + nx * ny * pair)
    rows = 2 + (ny - 1) + 2 + 1 + 2 + (ny - 1) + ny * over + ny * nx * pair
    return down + up, rows


def layer_kernel(
    dims, chunk, heads, nope, vd, scale,
    tokens, in_gain, wqd, wld, wrope, q_lat_gain, kv_lat_gain, wqu, wku, wvu, q_gain, k_gain, table, out_gain, w_out,
    out,
    normed, wqd_g, wld_g, wqu_g, wku_g, wvu_g, w_g, wq_s, wvt, kv_g, q_g, q_s, k_s, v_s, m_s, l_s, acc_s, scores, att_s, heads_g,
    send_sems, recv_sems, send_rows, recv_rows,
):
    nx, ny, nz, cores = dims
    seqs, dps = ny * nz, nx * cores
    rows = tokens.shape[0]
    s, d = lax.axis_index("sp"), lax.axis_index("dp")
    y, z = lax.rem(s, ny), lax.div(s, ny)
    c, x = lax.rem(d, cores), lax.div(d, cores)
    links = Links(send_sems, recv_sems, send_rows, recv_rows)

    def at_sp(target):
        return {"sp": target, "dp": d}

    def at_dp(target):
        return {"sp": s, "dp": target}

    def at_z(target):
        return at_sp(target * ny + y)

    def at_y(step):
        return at_sp(z * ny + lax.rem(y + step, ny))

    def at_x(step):
        return at_dp(lax.rem(x + step, nx) * cores + c)

    def at_core(step):
        return at_dp(x * cores + lax.rem(c + step, cores))

    def back_y(step):
        return lax.rem(y - step + ny, ny)

    def back_x(step):
        return lax.rem(x - step + nx, nx)

    def back_core(step):
        return lax.rem(c - step + cores, cores)

    def near(i):
        m = jnp.minimum(z, nz - 1 - z)
        two = i <= 2 * m
        dist = jnp.where(two, lax.div(i + 1, 2), i - m)
        up = jnp.where(two, lax.rem(i, 2) == 1, z < nz - 1 - z)
        return jnp.where(up, z + dist, z - dist)

    barrier = pltpu.get_barrier_semaphore()
    peers = [at_z(lax.rem(z + k, nz)) for k in range(1, nz)] + [at_y(k) for k in range(1, ny)]
    peers += [at_x(k) for k in range(1, nx)] + [at_core(k) for k in range(1, cores)]
    for peer in peers:
        pl.semaphore_signal(barrier, inc=1, device_id=peer, device_id_type=MESH)
    pl.semaphore_wait(barrier, len(peers))

    xs, ys, cs = range(1, nx), range(1, ny), range(1, cores)

    downs = ((wld, wld_g, DOWN_CUTS[0]), (wqd, wqd_g, DOWN_CUTS[1]))
    items = [(a, cut) for a in range(2) for cut in range(downs[a][2])]

    def piece(ref, a, cut, which):
        cuts = downs[a][2]
        part = ref.shape[0] // (ny * cuts)
        return ref.at[pl.ds(pl.multiple_of((which * cuts + cut) * part, part), part)]

    for it, (a, cut) in enumerate(items):
        src, dst, _ = downs[a]
        for dx in xs:
            links.send(("x", it, dx), piece(src, a, cut, y), piece(dst.at[d], a, cut, y), at_x(dx))
    for a, (src, dst, _) in enumerate(downs):
        for dc in cs:
            links.send(("c", a, dc), src, dst.at[d], at_core(dc))

    ups = ((wqu, wqu_g), (wku, wku_g), (wvu, wvu_g))
    for a, (src, dst) in enumerate(ups):
        for dy in ys:
            links.send(("uy", a, dy), src, dst.at[y, d], at_y(dy))
        for dc in cs:
            links.send(("uc", a, 0, 0, dc), src, dst.at[y, d], at_core(dc))

    part_out = w_out.shape[0]

    def w_block(zz, yy, xx, cc):
        first = ((zz * ny + yy) * dps + xx * cores + cc) * part_out
        return w_g.at[pl.ds(pl.multiple_of(first, part_out), part_out)]

    def along_z(role, way, origin, src, dst, ok):
        links.send((role, way), src, dst, at_z(jnp.clip(z + way, 0, nz - 1)), ok, at=origin)

    def z_arrival(step, way):
        origin = z - way * (step + 1)
        ok = (origin >= 0) & (origin < nz)
        return jnp.clip(origin, 0, nz - 1), ok, ok & (z + way >= 0) & (z + way < nz)

    def w_over_y(origin, src, ok):
        for dy in ys:
            links.send(("wy", dy), src, w_block(origin, y, x, c), at_y(dy), ok, at=origin)

    def w_over_x(origin, dyo, src, ok):
        for dx in xs:
            links.send(("wx", dyo, dx), src, w_block(origin, back_y(dyo), x, c), at_x(dx), ok, at=origin)

    def w_over_core(origin, dyo, dxo, src, ok):
        for dc in cs:
            dst = w_block(origin, back_y(dyo), back_x(dxo), c)
            links.send(("wc", dyo, dxo, dc), src, dst, at_core(dc), ok, at=origin)

    def w_z_relay(step, onward=True):
        for way in (1, -1):
            origin, ok, more = z_arrival(step, way)
            block = w_block(origin, y, x, c)
            links.arrive(("wz", way), block, at_sp(s), ok, at=origin)
            if onward:
                along_z("wz", way, origin, block, block, more)

    def w_z_onward(step):
        for way in (1, -1):
            origin, ok, more = z_arrival(step, way)
            block = w_block(origin, y, x, c)
            along_z("wz", way, origin, block, block, more)

    def w_z_spread(step):
        for way in (1, -1):
            origin, ok, _ = z_arrival(step, way)
            block = w_block(origin, y, x, c)
            w_over_x(origin, 0, block, ok)
            w_over_core(origin, 0, 0, block, ok)

    def w_y_near(k):
        origin = near(k)
        w_over_y(origin, w_block(origin, y, x, c), None)

    def w_y_copies(origin):
        copies = []
        for dy in ys:
            block = w_block(origin, back_y(dy), x, c)
            copies += [links.copy(("wx", dy, dx), origin, block, block, at_x(dx)) for dx in xs]
            copies += [links.copy(("wc", dy, 0, dc), origin, block, block, at_core(dc)) for dc in cs]
        return copies

    def w_y_service(origin):
        for dy in ys:
            links.arrive(("wy", dy), w_block(origin, back_y(dy), x, c), at_sp(s), at=origin)
        for copy in w_y_copies(origin):
            copy.start()

    def w_x_arrive(origin, dyo):
        for dx in xs:
            block = w_block(origin, back_y(dyo), back_x(dx), c)
            links.arrive(("wx", dyo, dx), block, at_dp(d), at=origin)
            w_over_core(origin, dyo, dx, block, None)

    own_block = w_block(z, y, x, c)
    for way in (1, -1):
        if nz > 1:
            along_z("wz", way, z, w_out, own_block, (z + way >= 0) & (z + way < nz))

    for src, dst, _ in downs:
        dst[d] = src[...]
    for src, dst in ups:
        dst[y, d] = src[...]
    own_out = pl.ds(pl.multiple_of((s * dps + d) * part_out, part_out), part_out)
    w_g[own_out, :] = w_out[...]

    def norm(i, _):
        step = rows // 4
        band = pl.ds(pl.multiple_of(i * step, step), step)
        normed[band, :] = rms_scale(tokens[band, :].astype(jnp.float32), in_gain[...]).astype(jnp.bfloat16)
        return 0

    lax.fori_loop(0, 4, norm, 0)
    rope_key = lax.dot_general(normed[...], wrope[...], NT, preferred_element_type=jnp.float32)
    kv_g[s, rows:, :] = pack_rope(rope_key)

    def down_x(it):
        a, cut = items[it]
        dst = downs[a][1]
        for dx in xs:
            got = piece(dst.at[back_x(dx) * cores + c], a, cut, y)
            links.arrive(("x", it, dx), got, at_dp(d))
            for dy in ys:
                links.send(("y", it, dx, dy), got, got, at_y(dy))
            for dc in cs:
                links.send(("cx", it, dx, dc), got, got, at_core(dc))

    def down_y(it):
        a, cut = items[it]
        dst = downs[a][1]
        for dx in xs:
            for dy in ys:
                got = piece(dst.at[back_x(dx) * cores + c], a, cut, back_y(dy))
                links.arrive(("y", it, dx, dy), got, at_dp(d))
                for dc in cs:
                    links.send(("cy", it, dx, dy, dc), got, got, at_core(dc))

    def settle_down(a):
        dst = downs[a][1]
        for dc in cs:
            links.arrive(("c", a, dc), dst.at[x * cores + back_core(dc)], at_dp(d))
            for it in range(len(items)):
                if items[it][0] != a:
                    continue
                for dx in xs:
                    origin = dst.at[back_x(dx) * cores + back_core(dc)]
                    links.arrive(("cx", it, dx, dc), piece(origin, a, items[it][1], y), at_dp(d))
                    for dy in ys:
                        got = piece(origin, a, items[it][1], back_y(dy))
                        links.arrive(("cy", it, dx, dy, dc), got, at_dp(d))

    def down(gathered):
        part = gathered.shape[1]
        total = None
        for k in range(dps):
            term = jnp.dot(normed[:, k * part : (k + 1) * part], gathered[k], preferred_element_type=jnp.float32)
            total = term if total is None else total + term
        return total

    def kv_over_y(zz, ok=None):
        block = kv_g.at[zz * ny + y]
        for dy in ys:
            links.send(("kvy", dy), block, block, at_y(dy), ok, at=zz)

    def launch(role, block):
        for way in (1, -1):
            if nz > 1:
                along_z(role, way, z, block, block, (z + way >= 0) & (z + way < nz))

    down_x(0)
    if nz > 1:
        w_z_relay(0)
    down_x(1)
    down_y(0)
    for it in range(2, len(items)):
        down_x(it)
    for a, (src, dst) in enumerate(ups):
        for dx in xs:
            links.send(("ux", a, 0, dx), src, dst.at[y, d], at_x(dx))
        for dy in ys:
            got = dst.at[back_y(dy), d]
            links.arrive(("uy", a, dy), got, at_dp(d))
            for dx in xs:
                links.send(("ux", a, dy, dx), got, got, at_x(dx))
            for dc in cs:
                links.send(("uc", a, dy, 0, dc), got, got, at_core(dc))
    settle_down(0)
    kv_g[s, :rows, :] = rms_scale(down(wld_g), kv_lat_gain[...]).astype(jnp.bfloat16)
    launch("kv", kv_g.at[s])
    kv_over_y(z)
    for it in range(1, len(items)):
        down_y(it)

    def up_spread(a):
        dst = ups[a][1]
        for dy in range(ny):
            for dx in xs:
                got = dst.at[back_y(dy), back_x(dx) * cores + c]
                links.arrive(("ux", a, dy, dx), got, at_dp(d))
                for dc in cs:
                    links.send(("uc", a, dy, dx, dc), got, got, at_core(dc))

    def settle_up(a):
        dst = ups[a][1]
        for dy in range(ny):
            for dx in range(nx):
                for dc in cs:
                    got = dst.at[back_y(dy), back_x(dx) * cores + back_core(dc)]
                    links.arrive(("uc", a, dy, dx, dc), got, at_dp(d))

    settle_down(1)
    q_g[z] = rms_scale(down(wqd_g), q_lat_gain[...]).astype(jnp.bfloat16)

    def z_relay(role, step, buffer, after=None, lazy=False):
        for way in (1, -1):
            origin, ok, more = z_arrival(step, way)
            block = buffer(origin)
            links.arrive((role, way), block, at_sp(s), more if lazy else ok, at=origin)
            along_z(role, way, origin, block, block, more)
            if after is not None:
                after(origin, ok)

    def kv_block(zz):
        return kv_g.at[zz * ny + y]

    for a in range(3):
        up_spread(a)
    if nz > 1:
        z_relay("kv", 0, kv_block, kv_over_y)
    w_over_x(z, 0, w_out, None)
    w_over_core(z, 0, 0, w_out, None)
    if nz > 1:
        w_z_spread(0)
    for a in range(3):
        settle_up(a)
    shard_heads = heads // ny
    depth = wqu.shape[0]
    for yy in range(ny):
        for k in range(dps):
            up = wqu_g[yy, k].astype(jnp.float32)
            width = wqu.shape[1] // shard_heads
            for h in range(shard_heads):
                head = up[:, h * width : (h + 1) * width]
                both = jnp.concatenate([head[:, :nope], with_swapped(head[:, nope:])], axis=1)
                wide = both.shape[1]
                first = (yy * shard_heads + h) * wide
                wq_s[k * depth : (k + 1) * depth, first : first + wide] = both.astype(jnp.bfloat16)
        wv = wvu_g[yy].reshape(dps * wvu.shape[0], wvu.shape[1])
        wvt[yy * shard_heads * vd : (yy + 1) * shard_heads * vd, :] = jnp.transpose(
            wv.astype(jnp.float32)
        ).astype(jnp.bfloat16)
    gq, gk = q_gain[:, :nope], k_gain[:, :nope]
    gq2, gk2 = with_swapped(q_gain[:, nope:]), with_swapped(k_gain[:, nope:])
    rope2 = gq2.shape[1]

    def project_kv(block):
        tok = pl.ds(pl.multiple_of(block * rows, rows), rows)
        wks = [wku_g[yy].reshape(dps * wku.shape[0], wku.shape[1]) for yy in range(ny)]
        shared = unpack_rope(kv_g[block, rows:, :], rope2)
        project_keys(block, rows, nope, kv_g[block, :rows, :], shared, wks, wvt, gk, table[tok, :] * gk2, k_s, v_s)

    def kv_column(zz):
        def one(j, _):
            yy = lax.rem(y + j, ny)
            project_kv(zz * ny + yy)
            return 0

        for dy in ys:
            links.arrive(("kvy", dy), kv_g.at[zz * ny + back_y(dy)], at_sp(s), at=zz)
        lax.fori_loop(0, ny, one, 0)

    def kv_columns(first, last):
        def one(i, _):
            kv_column(near(i))
            return 0

        lax.fori_loop(first, last, one, 0)


    def q_block(zz):
        return q_g.at[zz]

    for step in range(1, nz - 2):
        z_relay("kv", step, kv_block, kv_over_y)
    launch("q", q_g.at[z])
    kv_columns(0, 1)
    for step in range(max(nz - 2, 1), nz - 1):
        z_relay("kv", step, kv_block, kv_over_y)
    for step in range(1, nz - 2):
        w_z_relay(step, False)
        w_z_spread(step)
        z_relay("q", step - 1, q_block, lazy=True)
    for step in range(1, nz - 2):
        w_z_onward(step)
    w_over_y(z, w_out, None)
    for k in range(1, nz - 1):
        w_y_near(k)
    kv_columns(1, nz)
    w_y_service(z)

    def hand_over(zz):
        return links.copy("a2a", zz, att_s.at[zz], heads_g.at[z], at_z(zz), land=z)

    def attend(i, _):
        zz = near(i)
        low = zz < z
        last = jnp.where(low, z == nz - 1, z == 0)
        for way, side in ((1, low), (-1, zz > z)):
            links.arrive(("q", way), q_g.at[zz], at_sp(s), side & last, at=zz)
        qb = zz * ny + y
        tok = pl.ds(pl.multiple_of(qb * rows, rows), rows)
        project_queries(rows, heads, nope, q_g[zz], wq_s, gq, table[tok, :] * gq2, q_s)
        att_s[zz] = attend_block(zz, y, rows, chunk, heads, vd, scale, q_s, k_s, v_s, m_s, l_s, acc_s, scores)

        @pl.when(i > 0)
        def _():
            hand_over(zz).start()
        @pl.when((i > 0) & (i < nz - 2))
        def _():
            w_y_service(near(i + 1))

        return 0

    lax.fori_loop(0, 1, attend, 0)
    if nz > 1:
        w_y_service(near(1))
    for step in range(1, nz - 1):
        z_relay("q", step, q_block, lazy=True)
    for step in range(max(nz - 2, 1), nz - 1):
        w_z_relay(step, False)
        w_z_spread(step)
    if nz > 2:
        w_y_near(nz - 1)
    lax.fori_loop(1, max(nz - 1, 1), attend, 0)
    if nz > 2:
        w_y_service(near(nz - 1))
    lax.fori_loop(max(nz - 1, 1), nz, attend, 0)
    for k in range(nz):
        for dy in range(ny):
            w_x_arrive(lax.rem(z + k, nz), dy)
    heads_g[z] = att_s[z]
    for k in range(1, nz):
        origin = lax.rem(z + k, nz)
        links.copy("a2a", origin, att_s.at[origin], heads_g.at[z], at_z(origin), land=origin).wait_send()
        links.copy("a2a", origin, heads_g.at[origin], heads_g.at[origin], at_z(origin), land=origin).wait_recv()
    width = heads * vd
    square = jnp.zeros((rows, 1), jnp.float32)
    for k in range(nz):
        block = heads_g[k].astype(jnp.float32)
        square = square + jnp.sum(block * block, axis=-1, keepdims=True)
    r = lax.rsqrt(square * (1.0 / (nz * width)) + EPS)
    for k in range(nz):
        cols = slice(k * width, (k + 1) * width)
        normed[:, cols] = (heads_g[k].astype(jnp.float32) * r * out_gain[:, cols]).astype(jnp.bfloat16)
    for k in range(nz):
        origin = lax.rem(z + k, nz)
        for dy in range(ny):
            for dx in range(nx):
                for dc in cs:
                    block = w_block(origin, back_y(dy), back_x(dx), back_core(dc))
                    links.arrive(("wc", dy, dx, dc), block, at_dp(d), at=origin)
    tile = 256 if out.shape[1] % 256 == 0 else out.shape[1]

    def project_out(i, _):
        cols = pl.ds(pl.multiple_of(i * tile, tile), tile)
        out[:, cols] = jnp.dot(normed[...], w_g[:, cols], preferred_element_type=jnp.float32).astype(out.dtype)
        return 0

    lax.fori_loop(0, out.shape[1] // tile, project_out, 0)
    for k in range(nz):
        for copy in w_y_copies(lax.rem(z + k, nz)):
            copy.wait_send()
    links.drain()


def per_device(
    tokens, in_gain, w_query_down, w_latent_down, w_rope_key, query_latent_gain, latent_gain,
    w_query_up, w_key_up, w_value_up, query_gain, key_gain, out_gain, w_out,
):
    seqs, dps = lax.axis_size("sp"), lax.axis_size("dp")
    cores = 2 if dps % 2 == 0 else 1
    nx = dps // cores
    ny = nx if seqs % nx == 0 else 1
    nz = seqs // ny
    heads = HEADS // nz
    own_rows = tokens.shape[1]
    length = own_rows * seqs
    rope = w_rope_key.shape[1]
    nope = w_key_up.shape[1] * ny // heads
    vd = w_value_up.shape[1] * ny // heads
    wide = nope + 2 * rope
    chunk = ny * own_rows
    sems, sem_rows = sem_counts(nx, ny, nz, cores)
    b16 = jnp.bfloat16

    def gathered(w, *lead):
        return pltpu.VMEM(lead + (dps,) + w.shape, b16)

    result = pl.pallas_call(
        functools.partial(
            layer_kernel, (nx, ny, nz, cores), chunk, heads, nope, vd, float(nope + rope) ** -0.5
        ),
        out_shape=jax.ShapeDtypeStruct((own_rows, w_out.shape[1]), b16),
        in_specs=[pl.BlockSpec(memory_space=pltpu.VMEM)] * 15,
        out_specs=pl.BlockSpec(memory_space=pltpu.VMEM),
        scratch_shapes=[
            pltpu.VMEM((own_rows, max(tokens.shape[2], w_out.shape[0] * seqs * dps)), b16),
            gathered(w_query_down), gathered(w_latent_down),
            gathered(w_query_up, ny), gathered(w_key_up, ny), gathered(w_value_up, ny),
            pltpu.VMEM((w_out.shape[0] * seqs * dps, w_out.shape[1]), b16),
            pltpu.VMEM((w_query_down.shape[1], heads * wide), b16),
            pltpu.VMEM((heads * vd, w_latent_down.shape[1]), b16),
            pltpu.VMEM((seqs, own_rows + own_rows * rope // w_latent_down.shape[1], w_latent_down.shape[1]), b16),
            pltpu.VMEM((nz, own_rows, w_query_down.shape[1]), b16),
            pltpu.VMEM((heads, own_rows, wide), b16),
            pltpu.VMEM((heads, length, wide), b16),
            pltpu.VMEM((heads * vd, length), b16),
            pltpu.VMEM((heads, 1, own_rows), jnp.float32),
            pltpu.VMEM((heads, 1, own_rows), jnp.float32),
            pltpu.VMEM((heads, vd, own_rows), jnp.float32),
            pltpu.VMEM((heads, chunk, own_rows), jnp.float32),
            pltpu.VMEM((nz, own_rows, heads * vd), b16),
            pltpu.VMEM((nz, own_rows, heads * vd), b16),
            pltpu.SemaphoreType.DMA((sems,)),
            pltpu.SemaphoreType.DMA((sems,)),
            pltpu.SemaphoreType.DMA((sem_rows, nz)),
            pltpu.SemaphoreType.DMA((sem_rows, nz)),
        ],
        compiler_params=pltpu.CompilerParams(
            vmem_limit_bytes=56 * 1024 * 1024, collective_id=0, has_side_effects=True
        ),
        cost_estimate=pl.CostEstimate(flops=60 * 10**9, bytes_accessed=10**8, transcendentals=5 * 10**6),
    )(
        tokens.reshape(own_rows, tokens.shape[2]), in_gain[None], w_query_down, w_latent_down, w_rope_key.T,
        query_latent_gain[None], latent_gain[None], w_query_up, w_key_up, w_value_up,
        query_gain[None], key_gain[None], jnp.asarray(rotation_table(length, rope)), out_gain[None], w_out,
    )
    return result.reshape(1, own_rows, w_out.shape[1])


def solution(mesh):
    in_specs = (
        P("dp", "sp", None), P(), P("dp", None), P("dp", None), P(), P(), P(),
        P("dp", "sp"), P("dp", "sp"), P("dp", "sp"), P(), P(), P(), P(("sp", "dp"), None),
    )
    return jax.shard_map(
        per_device, mesh=mesh, in_specs=in_specs, out_specs=P("dp", "sp", None), check_vma=False
    )
```

```python
import functools

import jax
import jax.numpy as jnp
import numpy as np
from jax import lax
from jax.experimental import pallas as pl
from jax.experimental.pallas import tpu as pltpu
from jax.sharding import PartitionSpec as P

HEADS = 16
EPS = 1e-06
THETA = 10000.0
NEG_BIG = -1e30
LOG2E = 1.4426950408889634
NT = (((1,), (1,)), ((), ()))


def rms_scale(values, scaling):
    return values * lax.rsqrt(jnp.mean(values * values, axis=-1, keepdims=True) + EPS) * scaling


def swap_halves(x):
    half = x.shape[-1] // 2
    return jnp.concatenate([x[..., half:], x[..., :half]], axis=-1)


def rotation_table(length, width):
    half = width // 2
    frequency = np.float32(THETA) ** (-np.arange(half, dtype=np.float32) / np.float32(half))
    angles = np.arange(length, dtype=np.float32)[:, None] * frequency[None, :]
    cosine, sine = np.cos(angles), np.sin(angles)
    return np.concatenate([cosine, cosine, -sine, sine], axis=-1).astype(np.float32)


def with_swapped(x):
    return jnp.concatenate([x, swap_halves(x)], axis=-1)


def head_finish(t1, t2, r, gain, turn):
    rope2 = t2.shape[1]
    y = t2 * r * turn
    return (t1 * r * gain).astype(jnp.bfloat16), y + pltpu.roll(y, rope2 // 2, 1)


def project_queries(rows, heads, nope, lq, wq, gain, turn, q_s):
    wide = wq.shape[1] // heads
    rope2 = wide - nope
    inv = 1.0 / (nope + rope2 // 2)
    q = jnp.dot(lq, wq[...], preferred_element_type=jnp.float32)
    for h in range(heads):
        t1 = q[:, h * wide : h * wide + nope]
        t2 = q[:, h * wide + nope : (h + 1) * wide]
        r = lax.rsqrt(jnp.sum(t1 * t1 + 0.5 * t2 * t2, axis=-1, keepdims=True) * inv + EPS)
        first, last = head_finish(t1, t2, r, gain, turn)
        q_s[h, :, 0:nope] = first
        q_s[h, :, nope:wide] = last.astype(jnp.bfloat16)


def pack_rope(rope_key):
    part = rope_key.shape[0] // 4
    band = [rope_key[g * part : (g + 1) * part] for g in range(4)]
    return jnp.concatenate(band, axis=1).astype(jnp.bfloat16)


def unpack_rope(packed, rope2):
    quarter = rope2 // 4
    lane = lax.broadcasted_iota(jnp.int32, (packed.shape[0], rope2), 1)
    bands = []
    for g in range(4):
        p = packed[:, (g // 2) * rope2 : (g // 2 + 1) * rope2].astype(jnp.float32)
        if g % 2 == 0:
            front, b, a = p, pltpu.roll(p, quarter, 1), pltpu.roll(p, 3 * quarter, 1)
        else:
            front, b, a = pltpu.roll(p, 2 * quarter, 1), pltpu.roll(p, 3 * quarter, 1), pltpu.roll(p, quarter, 1)
        bands.append(jnp.where(lane < 2 * quarter, front, jnp.where(lane < 3 * quarter, b, a)))
    return jnp.concatenate(bands, axis=0)


def project_keys(block, rows, nope, lkv, shared, wks, wvt, gain, turn, k_s, v_s):
    tok = pl.ds(pl.multiple_of(block * rows, rows), rows)
    rope2 = shared.shape[1]
    wide = nope + rope2
    inv = 1.0 / (nope + rope2 // 2)
    v_s[:, tok] = lax.dot_general(wvt[...], lkv, NT, preferred_element_type=jnp.float32).astype(jnp.bfloat16)
    half_sq = 0.5 * shared * shared
    lane = lax.broadcasted_iota(jnp.int32, (rows, rope2), 1)
    turned = shared * turn
    turned = turned + pltpu.roll(turned, rope2 // 2, 1)
    turned = jnp.where(lane < rope2 // 2, turned, 0.0)
    h = 0
    for wk in wks:
        k = jnp.dot(lkv, wk, preferred_element_type=jnp.float32)
        for j in range(k.shape[1] // nope):
            t1 = k[:, j * nope : (j + 1) * nope]
            r = lax.rsqrt(jnp.sum(t1 * t1 + half_sq, axis=-1, keepdims=True) * inv + EPS)
            k_s[h, tok, 0:nope] = (t1 * r * gain).astype(jnp.bfloat16)
            k_s[h, tok, nope:wide] = (turned * r).astype(jnp.bfloat16)
            h += 1


def attend_item(j, y, rows, chunk, heads, vd, scale, masked, q_s, k_s, v_s, m_s, l_s, work):
    ktok = pl.ds(pl.multiple_of(j * chunk, chunk), chunk)
    factor = scale * LOG2E
    sub = 128

    def score_rows(h, first=0, count=chunk):
        return pl.ds(heads * vd + (h % 2) * chunk + first, count)

    def product(h):
        work[score_rows(h), :] = lax.dot_general(k_s[h, ktok, :], q_s[h], NT, preferred_element_type=jnp.float32)

    def band(h, first):
        s = work[score_rows(h, first, sub), :]
        if masked:
            kpos = first + lax.broadcasted_iota(jnp.int32, (sub, rows), 0)
            qpos = y * rows + lax.broadcasted_iota(jnp.int32, (sub, rows), 1)
            s = jnp.where(kpos <= qpos, s, NEG_BIG)
        return s

    product(0)
    for h in range(heads):
        if h + 1 < heads:
            product(h + 1)
        top = None
        for first in range(0, chunk, sub):
            part = jnp.max(band(h, first).reshape(sub // 8, 8, rows), axis=0)
            top = part if top is None else jnp.maximum(top, part)
        m = m_s[h]
        m_new = jnp.maximum(m, jnp.max(top, axis=0, keepdims=True) * factor)
        alpha = jnp.exp2(m - m_new)
        total, weights = None, []
        for first in range(0, chunk, sub):
            p = jnp.exp2(band(h, first) * factor - m_new)
            part = jnp.sum(p.reshape(sub // 8, 8, rows), axis=0)
            total = part if total is None else total + part
            weights.append(p.astype(jnp.bfloat16))
        m_s[h] = m_new
        l_s[h] = l_s[h] * alpha + jnp.sum(total, axis=0, keepdims=True)
        vt = v_s[h * vd : (h + 1) * vd, ktok]
        own = pl.ds(h * vd, vd)
        work[own, :] = work[own, :] * alpha + jnp.dot(
            vt, jnp.concatenate(weights, axis=0), preferred_element_type=jnp.float32
        )


def attend_block(i, y, rows, chunk, heads, vd, scale, q_s, k_s, v_s, m_s, l_s, work):
    m_s[...] = jnp.full(m_s.shape, NEG_BIG, jnp.float32)
    l_s[...] = jnp.zeros(l_s.shape, jnp.float32)
    work[0 : heads * vd, :] = jnp.zeros((heads * vd, rows), jnp.float32)

    def item(j, masked):
        attend_item(j, y, rows, chunk, heads, vd, scale, masked, q_s, k_s, v_s, m_s, l_s, work)

    def step(j, _):
        item(j, False)
        return 0

    lax.fori_loop(0, i, step, 0)
    item(i, True)
    return jnp.concatenate([jnp.transpose(work[h * vd : (h + 1) * vd, :] / l_s[h]) for h in range(heads)], axis=1).astype(jnp.bfloat16)


MESH = pl.DeviceIdType.MESH


class Links:
    def __init__(self, send_sems, recv_sems, send_rows, recv_rows):
        self.send_sems, self.recv_sems, self.ids, self.sent = send_sems, recv_sems, {}, []
        self.send_rows, self.recv_rows, self.row_ids = send_rows, recv_rows, {}

    def sems(self, role, at):
        if at is None:
            n = self.ids.setdefault(role, len(self.ids))
            return self.send_sems.at[n], self.recv_sems.at[n]
        n = self.row_ids.setdefault(role, len(self.row_ids))
        return self.send_rows.at[n, at], self.recv_rows.at[n, at]

    def copy(self, role, at, src, dst, target, land=None):
        send, recv = self.sems(role, at)
        if land is not None:
            recv = self.sems(role, land)[1]
        return pltpu.make_async_remote_copy(
            src_ref=src, dst_ref=dst, send_sem=send, recv_sem=recv, device_id=target, device_id_type=MESH,
        )

    def send(self, role, src, dst, target, ok=None, at=None):
        self.sent.append((ok, role, at, src, dst, target))
        guard(ok, lambda: self.copy(role, at, src, dst, target).start())

    def arrive(self, role, dst, target, ok=None, at=None):
        guard(ok, lambda: self.copy(role, at, dst, dst, target).wait_recv())

    def drain(self):
        for ok, role, at, src, dst, target in self.sent:
            guard(ok, lambda: self.copy(role, at, src, dst, target).wait_send())
        self.sent = []


def guard(ok, action):
    if ok is None:
        action()
    else:
        pl.when(ok)(action)


DOWN_CUTS = (1, 2)
TURNED = 2


def sem_counts(nx, ny, nz, cores, group):
    items = sum(DOWN_CUTS)
    over, pair = nx - 1, cores - 1
    down = items * over * ny * (1 + pair) + 2 * pair
    nzs = nz // group
    up = 3 * (nzs - 1 + nzs * (ny - 1) + nzs * ny * over + nzs * ny * nx * pair)
    rows = 2 + (ny - 1) + (group - 1) + 1 + 2 + (ny - 1) + ny * over + ny * nx * pair + over * (ny - 1)
    return down + up, rows


def layer_kernel(
    dims, chunk, heads, nope, vd, scale,
    tokens, in_gain, wqd, wld, wrope, q_lat_gain, kv_lat_gain, wqu, wku, wvu, q_gain, k_gain, table, out_gain, w_out,
    out,
    normed, wqd_g, wld_g, wqu_g, wku_g, wvu_g, w_g, wq_s, wvt, kv_g, q_g, q_s, k_s, v_s, m_s, l_s, work, att_s, heads_g,
    send_sems, recv_sems, send_rows, recv_rows,
):
    nx, ny, nz, cores, group = dims
    seqs, dps = ny * nz, nx * cores
    rows = tokens.shape[0]
    s, d = lax.axis_index("sp"), lax.axis_index("dp")
    y, z = lax.rem(s, ny), lax.div(s, ny)
    c, x = lax.rem(d, cores), lax.div(d, cores)
    zl, zo = lax.rem(z, group), lax.div(z, group)
    zb, nzs = z - zl, nz // group
    links = Links(send_sems, recv_sems, send_rows, recv_rows)

    def at_sp(target):
        return {"sp": target, "dp": d}

    def at_dp(target):
        return {"sp": s, "dp": target}

    def at_z(target):
        return at_sp(target * ny + y)

    def at_y(step):
        return at_sp(z * ny + lax.rem(y + step, ny))

    def at_x(step):
        return at_dp(lax.rem(x + step, nx) * cores + c)

    def at_core(step):
        return at_dp(x * cores + lax.rem(c + step, cores))

    def back_y(step):
        return lax.rem(y - step + ny, ny)

    def back_x(step):
        return lax.rem(x - step + nx, nx)

    def back_core(step):
        return lax.rem(c - step + cores, cores)

    def near(i):
        m = jnp.minimum(z, nz - 1 - z)
        two = i <= 2 * m
        dist = jnp.where(two, lax.div(i + 1, 2), i - m)
        up = jnp.where(two, lax.rem(i, 2) == 1, z < nz - 1 - z)
        return jnp.where(up, z + dist, z - dist)

    barrier = pltpu.get_barrier_semaphore()
    peers = [at_z(lax.rem(z + k, nz)) for k in range(1, nz)] + [at_y(k) for k in range(1, ny)]
    peers += [at_x(k) for k in range(1, nx)] + [at_core(k) for k in range(1, cores)]
    for peer in peers:
        pl.semaphore_signal(barrier, inc=1, device_id=peer, device_id_type=MESH)
    pl.semaphore_wait(barrier, len(peers))

    xs, ys, cs, zs = range(1, nx), range(1, ny), range(1, cores), range(1, nzs)

    downs = ((wld, wld_g, DOWN_CUTS[0]), (wqd, wqd_g, DOWN_CUTS[1]))
    items = [(a, cut) for a in range(2) for cut in range(downs[a][2])]

    def piece(ref, a, cut, which):
        cuts = downs[a][2]
        part = ref.shape[0] // (ny * cuts)
        return ref.at[pl.ds(pl.multiple_of((which * cuts + cut) * part, part), part)]

    for it, (a, cut) in enumerate(items):
        src, dst, _ = downs[a]
        for dx in xs:
            links.send(("x", it, dx), piece(src, a, cut, y), piece(dst.at[d], a, cut, y), at_x(dx))
    for a, (src, dst, _) in enumerate(downs):
        for dc in cs:
            links.send(("c", a, dc), src, dst.at[d], at_core(dc))

    ups = ((wqu, wqu_g), (wku, wku_g), (wvu, wvu_g))
    def up_slot(k, dy, dx, cc):
        return lax.rem(zo - k + nzs, nzs), back_y(dy), back_x(dx) * cores + cc

    def up_over_x(a, k, dy, src):
        dst = ups[a][1].at[up_slot(k, dy, 0, c)]
        for dx in xs:
            links.send(("ux", a, k, dy, dx), src, dst, at_x(dx))

    def up_over_y(a, k, src):
        dst = ups[a][1].at[up_slot(k, 0, 0, c)]
        for dy in ys:
            links.send(("uy", a, k, dy), src, dst, at_y(dy))

    def up_over_core(a, k, dy, dx, src):
        dst = ups[a][1].at[up_slot(k, dy, dx, c)]
        for dc in cs:
            links.send(("uc", a, k, dy, dx, dc), src, dst, at_core(dc))

    for a, (src, dst) in enumerate(ups):
        for k in zs:
            links.send(("uz", a, k), src, dst.at[zo, y, d], at_z(lax.rem(z + k * group, nz)))
        up_over_y(a, 0, src)
        up_over_x(a, 0, 0, src)
        up_over_core(a, 0, 0, 0, src)

    part_out = w_out.shape[0]

    def w_block(zz, yy, xx, cc):
        first = ((zz * ny + yy) * dps + xx * cores + cc) * part_out
        return w_g.at[pl.ds(pl.multiple_of(first, part_out), part_out)]

    def along_z(role, way, origin, src, dst, ok):
        links.send((role, way), src, dst, at_z(jnp.clip(z + way, 0, nz - 1)), ok, at=origin)

    def z_arrival(step, way):
        origin = z - way * (step + 1)
        ok = (origin >= 0) & (origin < nz)
        return jnp.clip(origin, 0, nz - 1), ok, ok & (z + way >= 0) & (z + way < nz)

    def w_over_y(origin, src, ok):
        for dy in ys:
            links.send(("wy", dy), src, w_block(origin, y, x, c), at_y(dy), ok, at=origin)

    def w_over_x(origin, dyo, src, ok):
        for dx in xs:
            links.send(("wx", dyo, dx), src, w_block(origin, back_y(dyo), x, c), at_x(dx), ok, at=origin)

    def w_over_core(origin, dyo, dxo, src, ok):
        for dc in cs:
            dst = w_block(origin, back_y(dyo), back_x(dxo), c)
            links.send(("wc", dyo, dxo, dc), src, dst, at_core(dc), ok, at=origin)

    def w_z_relay(step, onward=True):
        for way in (1, -1):
            origin, ok, more = z_arrival(step, way)
            block = w_block(origin, y, x, c)
            links.arrive(("wz", way), block, at_sp(s), ok, at=origin)
            if onward:
                along_z("wz", way, origin, block, block, more)

    def w_z_onward(step):
        for way in (1, -1):
            origin, ok, more = z_arrival(step, way)
            block = w_block(origin, y, x, c)
            along_z("wz", way, origin, block, block, more)

    def w_z_spread(step):
        for way in (1, -1):
            origin, ok, _ = z_arrival(step, way)
            block = w_block(origin, y, x, c)
            w_over_x(origin, 0, block, ok)
            w_over_core(origin, 0, 0, block, ok)

    def w_y_near(k):
        origin = near(k)
        w_over_y(origin, w_block(origin, y, x, c), None)

    def w_y_copies(origin, turned):
        copies = []
        for dy in ys:
            block = w_block(origin, back_y(dy), x, c)
            if not turned:
                copies += [links.copy(("wx", dy, dx), origin, block, block, at_x(dx)) for dx in xs]
            copies += [links.copy(("wc", dy, 0, dc), origin, block, block, at_core(dc)) for dc in cs]
        return copies

    def w_y_service(origin, turned=False):
        for dy in ys:
            links.arrive(("wy", dy), w_block(origin, back_y(dy), x, c), at_sp(s), at=origin)
        for copy in w_y_copies(origin, turned):
            copy.start()

    def w_x_turn(origin):
        for dx in xs:
            block = w_block(origin, y, back_x(dx), c)
            links.arrive(("wx", 0, dx), block, at_dp(d), at=origin)
            w_over_core(origin, 0, dx, block, None)
            for dy in ys:
                links.send(("wxy", dx, dy), block, block, at_y(dy), at=origin)

    def w_turned(origin):
        for dx in xs:
            for dy in ys:
                block = w_block(origin, back_y(dy), back_x(dx), c)
                links.arrive(("wxy", dx, dy), block, at_dp(d), at=origin)
                w_over_core(origin, dy, dx, block, None)

    def w_x_arrive(origin, dyo):
        for dx in xs:
            block = w_block(origin, back_y(dyo), back_x(dx), c)
            links.arrive(("wx", dyo, dx), block, at_dp(d), at=origin)
            w_over_core(origin, dyo, dx, block, None)

    own_block = w_block(z, y, x, c)
    for way in (1, -1):
        if nz > 1:
            along_z("wz", way, z, w_out, own_block, (z + way >= 0) & (z + way < nz))

    for src, dst, _ in downs:
        dst[d] = src[...]
    for src, dst in ups:
        dst[zo, y, d] = src[...]
    own_out = pl.ds(pl.multiple_of((s * dps + d) * part_out, part_out), part_out)
    w_g[own_out, :] = w_out[...]

    def norm(i, _):
        step = rows // 4
        band = pl.ds(pl.multiple_of(i * step, step), step)
        normed[band, :] = rms_scale(tokens[band, :].astype(jnp.float32), in_gain[...]).astype(jnp.bfloat16)
        return 0

    lax.fori_loop(0, 4, norm, 0)
    rope_key = lax.dot_general(normed[...], wrope[...], NT, preferred_element_type=jnp.float32)
    kv_g[s, rows:, :] = pack_rope(rope_key)

    def down_x(it):
        a, cut = items[it]
        dst = downs[a][1]
        for dx in xs:
            got = piece(dst.at[back_x(dx) * cores + c], a, cut, y)
            links.arrive(("x", it, dx), got, at_dp(d))
            for dy in ys:
                links.send(("y", it, dx, dy), got, got, at_y(dy))
            for dc in cs:
                links.send(("cx", it, dx, dc), got, got, at_core(dc))

    def down_y(it):
        a, cut = items[it]
        dst = downs[a][1]
        for dx in xs:
            for dy in ys:
                got = piece(dst.at[back_x(dx) * cores + c], a, cut, back_y(dy))
                links.arrive(("y", it, dx, dy), got, at_dp(d))
                for dc in cs:
                    links.send(("cy", it, dx, dy, dc), got, got, at_core(dc))

    def settle_down(a):
        dst = downs[a][1]
        for dc in cs:
            links.arrive(("c", a, dc), dst.at[x * cores + back_core(dc)], at_dp(d))
            for it in range(len(items)):
                if items[it][0] != a:
                    continue
                for dx in xs:
                    origin = dst.at[back_x(dx) * cores + back_core(dc)]
                    links.arrive(("cx", it, dx, dc), piece(origin, a, items[it][1], y), at_dp(d))
                    for dy in ys:
                        got = piece(origin, a, items[it][1], back_y(dy))
                        links.arrive(("cy", it, dx, dy, dc), got, at_dp(d))

    def down(gathered):
        part = gathered.shape[1]
        total = None
        for k in range(dps):
            term = jnp.dot(normed[:, k * part : (k + 1) * part], gathered[k], preferred_element_type=jnp.float32)
            total = term if total is None else total + term
        return total

    def kv_over_y(zz, ok=None):
        block = kv_g.at[zz * ny + y]
        for dy in ys:
            links.send(("kvy", dy), block, block, at_y(dy), ok, at=zz)

    def up_arrive(role, a, k, dy, dx):
        got = ups[a][1].at[up_slot(k, dy, dx, c)]
        links.arrive(role, got, at_dp(d))
        return got

    down_x(0)
    down_x(1)
    down_y(0)
    for a in range(3):
        for dy in ys:
            got = up_arrive(("uy", a, 0, dy), a, 0, dy, 0)
            up_over_x(a, 0, dy, got)
            up_over_core(a, 0, dy, 0, got)
    for it in range(2, len(items)):
        down_x(it)
    def up_z(a):
        for k in zs:
            got = up_arrive(("uz", a, k), a, k, 0, 0)
            up_over_y(a, k, got)
            up_over_x(a, k, 0, got)
            up_over_core(a, k, 0, 0, got)

    settle_down(0)
    kv_g[s, :rows, :] = rms_scale(down(wld_g), kv_lat_gain[...]).astype(jnp.bfloat16)
    own_kv = kv_g.at[s]
    along_z("kv", 1, z, own_kv, own_kv, z < nz - 1)
    along_z("kv", -1, z, own_kv, own_kv, z > zb)
    kv_over_y(z)
    for it in range(1, len(items)):
        down_y(it)

    def up_diagonal(a):
        for k in zs:
            for dy in ys:
                got = up_arrive(("uy", a, k, dy), a, k, dy, 0)
                up_over_x(a, k, dy, got)
                up_over_core(a, k, dy, 0, got)

    def up_spread(a, k):
        for dy in range(ny):
            for dx in xs:
                up_over_core(a, k, dy, dx, up_arrive(("ux", a, k, dy, dx), a, k, dy, dx))

    def settle_up(a):
        for k in range(nzs):
            for dy in range(ny):
                for dx in range(nx):
                    for dc in cs:
                        got = ups[a][1].at[up_slot(k, dy, dx, back_core(dc))]
                        links.arrive(("uc", a, k, dy, dx, dc), got, at_dp(d))

    settle_down(1)
    q_g[zl] = rms_scale(down(wqd_g), q_lat_gain[...]).astype(jnp.bfloat16)

    def kv_relay(step):
        for way in (1, -1):
            origin, ok, more = z_arrival(step, way)
            if way < 0:
                base = origin - lax.rem(origin, group)
                ok, more = ok & (z >= base), more & (z - 1 >= base)
            block = kv_g.at[origin * ny + y]
            links.arrive(("kv", way), block, at_sp(s), ok, at=origin)
            along_z("kv", way, origin, block, block, more)
            kv_over_y(origin, ok)

    for a in range(3):
        up_z(a)
    if nz > 1:
        kv_relay(0)
    if nz > 1:
        w_z_relay(0)
    for a in range(3):
        up_diagonal(a)
    for step in range(1, nz - 2):
        kv_relay(step)
    for k in range(1, group):
        links.send(("q", k), q_g.at[zl], q_g.at[zl], at_z(zb + lax.rem(zl + k, group)), at=zl)
    w_over_x(z, 0, w_out, None)
    w_over_core(z, 0, 0, w_out, None)
    if nz > 1:
        w_z_spread(0)
    w_over_y(z, w_out, None)
    for a in range(3):
        up_spread(a, 0)
    for k in zs:
        for a in range(3):
            up_spread(a, k)
    for a in range(3):
        settle_up(a)
    for step in range(max(nz - 2, 1), nz - 1):
        kv_relay(step)
    for k in range(1, min(2, nz)):
        w_y_near(k)
    for step in range(1, nz - 2):
        w_z_relay(step)
        w_z_spread(step)
    for k in range(2, nz - 1):
        w_y_near(k)
    shards = nzs * ny
    shard_heads = heads // shards
    depth = wqu.shape[0]
    for yy in range(shards):
        for k in range(dps):
            up = wqu_g[yy // ny, yy % ny, k].astype(jnp.float32)
            width = wqu.shape[1] // shard_heads
            for h in range(shard_heads):
                head = up[:, h * width : (h + 1) * width]
                both = jnp.concatenate([head[:, :nope], with_swapped(head[:, nope:])], axis=1)
                wide = both.shape[1]
                first = (yy * shard_heads + h) * wide
                wq_s[k * depth : (k + 1) * depth, first : first + wide] = both.astype(jnp.bfloat16)
        wv = wvu_g[yy // ny, yy % ny].reshape(dps * wvu.shape[0], wvu.shape[1])
        wvt[yy * shard_heads * vd : (yy + 1) * shard_heads * vd, :] = jnp.transpose(
            wv.astype(jnp.float32)
        ).astype(jnp.bfloat16)
    gq, gk = q_gain[:, :nope], k_gain[:, :nope]
    gq2, gk2 = with_swapped(q_gain[:, nope:]), with_swapped(k_gain[:, nope:])
    rope2 = gq2.shape[1]

    def project_kv(block):
        tok = pl.ds(pl.multiple_of(block * rows, rows), rows)
        wks = [wku_g[yy // ny, yy % ny].reshape(dps * wku.shape[0], wku.shape[1]) for yy in range(shards)]
        shared = unpack_rope(kv_g[block, rows:, :], rope2)
        project_keys(block, rows, nope, kv_g[block, :rows, :], shared, wks, wvt, gk, table[tok, :] * gk2, k_s, v_s)

    def kv_column(zz):
        def one(j, _):
            yy = lax.rem(y + j, ny)
            project_kv(zz * ny + yy)
            return 0

        for dy in ys:
            links.arrive(("kvy", dy), kv_g.at[zz * ny + back_y(dy)], at_sp(s), at=zz)
        lax.fori_loop(0, ny, one, 0)

    def kv_columns(first, last):
        def one(i, _):
            inside = zb + lax.rem(zl + i, group)
            kv_column(jnp.where(i < group, inside, zb - 1 - (i - group)))
            return 0

        lax.fori_loop(first, last, one, 0)

    kv_columns(0, 1)
    kv_columns(1, zb + group)
    def hand_over(li):
        return links.copy("a2a", li, att_s.at[li], heads_g.at[zl], at_z(zb + li), land=zl)

    def attend(i, _):
        li = lax.rem(zl + 1 + i, group)
        for k in range(1, group):
            links.arrive(("q", k), q_g.at[li], at_sp(s), li == lax.rem(zl - k + group, group), at=li)
        zz = zb + li
        qb = zz * ny + y
        tok = pl.ds(pl.multiple_of(qb * rows, rows), rows)
        project_queries(rows, heads, nope, q_g[li], wq_s, gq, table[tok, :] * gq2, q_s)
        att_s[li] = attend_block(zz, y, rows, chunk, heads, vd, scale, q_s, k_s, v_s, m_s, l_s, work)

        @pl.when(i < group - 1)
        def _():
            hand_over(li).start()

        @pl.when(i == 0)
        def _():
            for k in range(2, nz):
                w_y_service(near(k), k < TURNED)

        return 0

    for step in range(max(nz - 2, 1), nz - 1):
        w_z_relay(step, False)
        w_z_spread(step)
    if nz > 2:
        w_y_near(nz - 1)

    for k in range(min(TURNED, nz)):
        w_x_turn(near(k))
    w_y_service(z, TURNED > 0)
    if nz > 1:
        w_y_service(near(1), TURNED > 1)
    lax.fori_loop(0, group, attend, 0)
    heads_g[zl] = att_s[zl]
    for k in range(1, group):
        li = lax.rem(zl + k, group)
        hand_over(li).wait_send()
        links.copy("a2a", li, heads_g.at[li], heads_g.at[li], at_z(zb + li), land=li).wait_recv()
    width = heads * vd
    band = width // nzs
    square = jnp.zeros((rows, 1), jnp.float32)
    for k in range(group):
        block = heads_g[k].astype(jnp.float32)
        square = square + jnp.sum(block * block, axis=-1, keepdims=True)
    r = lax.rsqrt(square * (1.0 / (group * width)) + EPS)
    for k in range(group):
        for j in range(nzs):
            cols = slice((j * group + k) * band, (j * group + k + 1) * band)
            part = heads_g[k, :, j * band : (j + 1) * band].astype(jnp.float32)
            normed[:, cols] = (part * r * out_gain[:, cols]).astype(jnp.bfloat16)
    for k in range(nz):
        if k >= TURNED:
            w_x_arrive(near(k), 0)

    def settle_w(dy):
        for k in range(nz):
            for dx in range(nx):
                for dc in cs:
                    block = w_block(near(k), back_y(dy), back_x(dx), back_core(dc))
                    links.arrive(("wc", dy, dx, dc), block, at_dp(d), at=near(k))

    settle_w(0)
    tile = rows * max(1, 512 // rows)
    run = dps * part_out

    def partial_out(yy, cols):
        total = None
        for zz in range(nz):
            first = pl.multiple_of((zz * ny + yy) * run, run)
            term = jnp.dot(normed[:, pl.ds(first, run)], w_g[pl.ds(first, run), cols], preferred_element_type=jnp.float32)
            total = term if total is None else total + term
        return total

    def project_own(i, _):
        cols = pl.ds(pl.multiple_of(i * tile, tile), tile)
        total = partial_out(y, cols)
        for j in range(tile // rows):
            at = pl.multiple_of(i * tile + j * rows, rows)
            work[pl.ds(at, rows), :] = total[:, j * rows : (j + 1) * rows]
        return 0

    lax.fori_loop(0, out.shape[1] // tile, project_own, 0)
    for k in range(nz):
        if k < TURNED:
            w_turned(near(k))
            continue
        for dy in ys:
            w_x_arrive(near(k), dy)
    for dy in ys:
        settle_w(dy)

    def project_rest(i, _):
        cols = pl.ds(pl.multiple_of(i * tile, tile), tile)
        at = pl.multiple_of(i * tile, tile)
        total = jnp.concatenate([work[pl.ds(at + j * rows, rows), :] for j in range(tile // rows)], axis=1)
        for dy in ys:
            total = total + partial_out(back_y(dy), cols)
        out[:, cols] = total.astype(out.dtype)
        return 0

    lax.fori_loop(0, out.shape[1] // tile, project_rest, 0)
    for k in range(nz):
        for copy in w_y_copies(near(k), k < TURNED):
            copy.wait_send()
    links.drain()


def per_device(
    tokens, in_gain, w_query_down, w_latent_down, w_rope_key, query_latent_gain, latent_gain,
    w_query_up, w_key_up, w_value_up, query_gain, key_gain, out_gain, w_out,
):
    seqs, dps = lax.axis_size("sp"), lax.axis_size("dp")
    cores = 2 if dps % 2 == 0 else 1
    nx = dps // cores
    ny = nx if seqs % nx == 0 else 1
    nz = seqs // ny
    group = 2 if nz % 2 == 0 else nz
    heads = HEADS // group
    shards = seqs // group
    own_rows = tokens.shape[1]
    length = own_rows * seqs
    rope = w_rope_key.shape[1]
    nope = w_key_up.shape[1] * shards // heads
    vd = w_value_up.shape[1] * shards // heads
    wide = nope + 2 * rope
    chunk = ny * own_rows
    sems, sem_rows = sem_counts(nx, ny, nz, cores, group)
    b16 = jnp.bfloat16

    def gathered(w, *lead):
        return pltpu.VMEM(lead + (dps,) + w.shape, b16)

    result = pl.pallas_call(
        functools.partial(
            layer_kernel, (nx, ny, nz, cores, group), chunk, heads, nope, vd, float(nope + rope) ** -0.5
        ),
        out_shape=jax.ShapeDtypeStruct((own_rows, w_out.shape[1]), b16),
        in_specs=[pl.BlockSpec(memory_space=pltpu.VMEM)] * 15,
        out_specs=pl.BlockSpec(memory_space=pltpu.VMEM),
        scratch_shapes=[
            pltpu.VMEM((own_rows, max(tokens.shape[2], w_out.shape[0] * seqs * dps)), b16),
            gathered(w_query_down), gathered(w_latent_down),
            gathered(w_query_up, nz // group, ny), gathered(w_key_up, nz // group, ny), gathered(w_value_up, nz // group, ny),
            pltpu.VMEM((w_out.shape[0] * seqs * dps, w_out.shape[1]), b16),
            pltpu.VMEM((w_query_down.shape[1], heads * wide), b16),
            pltpu.VMEM((heads * vd, w_latent_down.shape[1]), b16),
            pltpu.VMEM((seqs, own_rows + own_rows * rope // w_latent_down.shape[1], w_latent_down.shape[1]), b16),
            pltpu.VMEM((group, own_rows, w_query_down.shape[1]), b16),
            pltpu.VMEM((heads, own_rows, wide), b16),
            pltpu.VMEM((heads, length, wide), b16),
            pltpu.VMEM((heads * vd, length), b16),
            pltpu.VMEM((heads, 1, own_rows), jnp.float32),
            pltpu.VMEM((heads, 1, own_rows), jnp.float32),
            pltpu.VMEM((max(heads * vd + 2 * chunk, w_out.shape[1]), own_rows), jnp.float32),
            pltpu.VMEM((group, own_rows, heads * vd), b16),
            pltpu.VMEM((group, own_rows, heads * vd), b16),
            pltpu.SemaphoreType.DMA((sems,)),
            pltpu.SemaphoreType.DMA((sems,)),
            pltpu.SemaphoreType.DMA((sem_rows, nz)),
            pltpu.SemaphoreType.DMA((sem_rows, nz)),
        ],
        compiler_params=pltpu.CompilerParams(
            vmem_limit_bytes=62 * 1024 * 1024, collective_id=0, has_side_effects=True
        ),
        cost_estimate=pl.CostEstimate(flops=60 * 10**9, bytes_accessed=10**8, transcendentals=5 * 10**6),
    )(
        tokens.reshape(own_rows, tokens.shape[2]), in_gain[None], w_query_down, w_latent_down, w_rope_key.T,
        query_latent_gain[None], latent_gain[None], w_query_up, w_key_up, w_value_up,
        query_gain[None], key_gain[None], jnp.asarray(rotation_table(length, rope)), out_gain[None], w_out,
    )
    return result.reshape(1, own_rows, w_out.shape[1])


def solution(mesh):
    in_specs = (
        P("dp", "sp", None), P(), P("dp", None), P("dp", None), P(), P(), P(),
        P("dp", "sp"), P("dp", "sp"), P("dp", "sp"), P(), P(), P(), P(("sp", "dp"), None),
    )
    return jax.shard_map(
        per_device, mesh=mesh, in_specs=in_specs, out_specs=P("dp", "sp", None), check_vma=False
    )
```

```python
import functools

import jax
import jax.numpy as jnp
import numpy as np
from jax import lax
from jax.experimental import pallas as pl
from jax.experimental.pallas import tpu as pltpu
from jax.sharding import PartitionSpec as P

HEADS = 16
EPS = 1e-06
THETA = 10000.0
NEG_BIG = -1e30
LOG2E = 1.4426950408889634
NT = (((1,), (1,)), ((), ()))


def rms_scale(values, scaling):
    return values * lax.rsqrt(jnp.mean(values * values, axis=-1, keepdims=True) + EPS) * scaling


def swap_halves(x):
    half = x.shape[-1] // 2
    return jnp.concatenate([x[..., half:], x[..., :half]], axis=-1)


def rotation_table(length, width):
    half = width // 2
    frequency = np.float32(THETA) ** (-np.arange(half, dtype=np.float32) / np.float32(half))
    angles = np.arange(length, dtype=np.float32)[:, None] * frequency[None, :]
    cosine, sine = np.cos(angles), np.sin(angles)
    return np.concatenate([cosine, cosine, -sine, sine], axis=-1).astype(np.float32)


def with_swapped(x):
    return jnp.concatenate([x, swap_halves(x)], axis=-1)


def head_finish(t1, t2, r, gain, turn):
    rope2 = t2.shape[1]
    y = t2 * r * turn
    return (t1 * r * gain).astype(jnp.bfloat16), y + pltpu.roll(y, rope2 // 2, 1)


def project_queries(rows, heads, nope, lq, wq, gain, turn, q_s):
    wide = wq.shape[1] // heads
    rope2 = wide - nope
    inv = 1.0 / (nope + rope2 // 2)
    q = jnp.dot(lq, wq[...], preferred_element_type=jnp.float32)
    for h in range(heads):
        t1 = q[:, h * wide : h * wide + nope]
        t2 = q[:, h * wide + nope : (h + 1) * wide]
        r = lax.rsqrt(jnp.sum(t1 * t1 + 0.5 * t2 * t2, axis=-1, keepdims=True) * inv + EPS)
        first, last = head_finish(t1, t2, r, gain, turn)
        q_s[h, :, 0:nope] = first
        q_s[h, :, nope:wide] = last.astype(jnp.bfloat16)


def pack_rope(rope_key):
    part = rope_key.shape[0] // 4
    band = [rope_key[g * part : (g + 1) * part] for g in range(4)]
    return jnp.concatenate(band, axis=1).astype(jnp.bfloat16)


def unpack_rope(packed, rope2):
    quarter = rope2 // 4
    lane = lax.broadcasted_iota(jnp.int32, (packed.shape[0], rope2), 1)
    bands = []
    for g in range(4):
        p = packed[:, (g // 2) * rope2 : (g // 2 + 1) * rope2].astype(jnp.float32)
        if g % 2 == 0:
            front, b, a = p, pltpu.roll(p, quarter, 1), pltpu.roll(p, 3 * quarter, 1)
        else:
            front, b, a = pltpu.roll(p, 2 * quarter, 1), pltpu.roll(p, 3 * quarter, 1), pltpu.roll(p, quarter, 1)
        bands.append(jnp.where(lane < 2 * quarter, front, jnp.where(lane < 3 * quarter, b, a)))
    return jnp.concatenate(bands, axis=0)


def project_keys(block, rows, nope, lkv, shared, wks, wvt, gain, turn, k_s, v_s):
    tok = pl.ds(pl.multiple_of(block * rows, rows), rows)
    rope2 = shared.shape[1]
    wide = nope + rope2
    inv = 1.0 / (nope + rope2 // 2)
    v_s[:, tok] = lax.dot_general(wvt[...], lkv, NT, preferred_element_type=jnp.float32).astype(jnp.bfloat16)
    half_sq = 0.5 * shared * shared
    lane = lax.broadcasted_iota(jnp.int32, (rows, rope2), 1)
    turned = shared * turn
    turned = turned + pltpu.roll(turned, rope2 // 2, 1)
    turned = jnp.where(lane < rope2 // 2, turned, 0.0)
    h = 0
    for wk in wks:
        k = jnp.dot(lkv, wk, preferred_element_type=jnp.float32)
        for j in range(k.shape[1] // nope):
            t1 = k[:, j * nope : (j + 1) * nope]
            r = lax.rsqrt(jnp.sum(t1 * t1 + half_sq, axis=-1, keepdims=True) * inv + EPS)
            k_s[h, tok, 0:nope] = (t1 * r * gain).astype(jnp.bfloat16)
            k_s[h, tok, nope:wide] = (turned * r).astype(jnp.bfloat16)
            h += 1


def attend_item(j, y, rows, chunk, heads, vd, scale, masked, q_s, k_s, v_s, m_s, l_s, work):
    ktok = pl.ds(pl.multiple_of(j * chunk, chunk), chunk)
    factor = scale * LOG2E
    sub = 128

    def score_rows(h, first=0, count=chunk):
        return pl.ds(heads * vd + (h % 2) * chunk + first, count)

    def product(h):
        work[score_rows(h), :] = lax.dot_general(k_s[h, ktok, :], q_s[h], NT, preferred_element_type=jnp.float32)

    def band(h, first):
        s = work[score_rows(h, first, sub), :]
        if masked:
            kpos = first + lax.broadcasted_iota(jnp.int32, (sub, rows), 0)
            qpos = y * rows + lax.broadcasted_iota(jnp.int32, (sub, rows), 1)
            s = jnp.where(kpos <= qpos, s, NEG_BIG)
        return s

    product(0)
    for h in range(heads):
        if h + 1 < heads:
            product(h + 1)
        top = None
        for first in range(0, chunk, sub):
            part = jnp.max(band(h, first).reshape(sub // 8, 8, rows), axis=0)
            top = part if top is None else jnp.maximum(top, part)
        m = m_s[h]
        m_new = jnp.maximum(m, jnp.max(top, axis=0, keepdims=True) * factor)
        alpha = jnp.exp2(m - m_new)
        total, weights = None, []
        for first in range(0, chunk, sub):
            p = jnp.exp2(band(h, first) * factor - m_new)
            part = jnp.sum(p.reshape(sub // 8, 8, rows), axis=0)
            total = part if total is None else total + part
            weights.append(p.astype(jnp.bfloat16))
        m_s[h] = m_new
        l_s[h] = l_s[h] * alpha + jnp.sum(total, axis=0, keepdims=True)
        vt = v_s[h * vd : (h + 1) * vd, ktok]
        own = pl.ds(h * vd, vd)
        work[own, :] = work[own, :] * alpha + jnp.dot(
            vt, jnp.concatenate(weights, axis=0), preferred_element_type=jnp.float32
        )


def attend_block(i, y, rows, chunk, heads, vd, scale, q_s, k_s, v_s, m_s, l_s, work, between):
    m_s[...] = jnp.full(m_s.shape, NEG_BIG, jnp.float32)
    l_s[...] = jnp.zeros(l_s.shape, jnp.float32)
    work[0 : heads * vd, :] = jnp.zeros((heads * vd, rows), jnp.float32)

    def item(j, masked):
        attend_item(j, y, rows, chunk, heads, vd, scale, masked, q_s, k_s, v_s, m_s, l_s, work)

    def step(j, _):
        item(j, False)
        return 0

    lax.fori_loop(0, i, step, 0)
    between()
    item(i, True)
    return jnp.concatenate([jnp.transpose(work[h * vd : (h + 1) * vd, :] / l_s[h]) for h in range(heads)], axis=1).astype(jnp.bfloat16)


MESH = pl.DeviceIdType.MESH


class Links:
    def __init__(self, send_sems, recv_sems, send_rows, recv_rows):
        self.send_sems, self.recv_sems, self.ids, self.sent = send_sems, recv_sems, {}, []
        self.send_rows, self.recv_rows, self.row_ids = send_rows, recv_rows, {}

    def sems(self, role, at):
        if at is None:
            n = self.ids.setdefault(role, len(self.ids))
            return self.send_sems.at[n], self.recv_sems.at[n]
        n = self.row_ids.setdefault(role, len(self.row_ids))
        return self.send_rows.at[n, at], self.recv_rows.at[n, at]

    def copy(self, role, at, src, dst, target, land=None):
        send, recv = self.sems(role, at)
        if land is not None:
            recv = self.sems(role, land)[1]
        return pltpu.make_async_remote_copy(
            src_ref=src, dst_ref=dst, send_sem=send, recv_sem=recv, device_id=target, device_id_type=MESH,
        )

    def send(self, role, src, dst, target, ok=None, at=None):
        self.sent.append((ok, role, at, src, dst, target))
        guard(ok, lambda: self.copy(role, at, src, dst, target).start())

    def arrive(self, role, dst, target, ok=None, at=None):
        guard(ok, lambda: self.copy(role, at, dst, dst, target).wait_recv())

    def drain(self):
        for ok, role, at, src, dst, target in self.sent:
            guard(ok, lambda: self.copy(role, at, src, dst, target).wait_send())
        self.sent = []


def guard(ok, action):
    if ok is None:
        action()
    else:
        pl.when(ok)(action)


DOWN_CUTS = (1, 2)
TURNED = 1


def sem_counts(nx, ny, nz, cores, group):
    items = sum(DOWN_CUTS)
    over, pair = nx - 1, cores - 1
    down = items * over * ny * (1 + pair) + 2 * pair
    nzs = nz // group
    up = 3 * (nzs - 1 + nzs * (ny - 1) + nzs * ny * over + nzs * ny * nx * pair)
    rows = 2 + (ny - 1) + (group - 1) + 1 + 2 + (ny - 1) + ny * over + ny * nx * pair + over * (ny - 1)
    return down + up, rows


def layer_kernel(
    dims, chunk, heads, nope, vd, scale,
    tokens_in, in_gain_in, wqd_in, wld_in, wrope_in, q_lat_gain_in, kv_lat_gain_in, wqu_in, wku_in, wvu_in,
    q_gain_in, k_gain_in, table_in, out_gain_in, w_out_in,
    out,
    in_gain, wrope, q_lat_gain, kv_lat_gain, q_gain, k_gain, table, out_gain,
    normed, wqd_g, wld_g, wqu_g, wku_g, wvu_g, w_g, wq_s, wvt, kv_g, q_g, q_s, k_s, v_s, m_s, l_s, work, att_s, heads_g,
    send_sems, recv_sems, send_rows, recv_rows, load_sems,
):
    nx, ny, nz, cores, group = dims
    seqs, dps = ny * nz, nx * cores
    rows = tokens_in.shape[0]
    s, d = lax.axis_index("sp"), lax.axis_index("dp")
    y, z = lax.rem(s, ny), lax.div(s, ny)
    c, x = lax.rem(d, cores), lax.div(d, cores)
    zl, zo = lax.rem(z, group), lax.div(z, group)
    zb, nzs = z - zl, nz // group
    links = Links(send_sems, recv_sems, send_rows, recv_rows)

    part_out = w_out_in.shape[0]

    def w_block(zz, yy, xx, cc):
        first = ((zz * ny + yy) * dps + xx * cores + cc) * part_out
        return w_g.at[pl.ds(pl.multiple_of(first, part_out), part_out)]

    wqd, wld, w_out = wqd_g.at[d], wld_g.at[d], w_block(z, y, x, c)
    wqu, wku, wvu = wqu_g.at[zo, y, d], wku_g.at[zo, y, d], wvu_g.at[zo, y, d]
    pairs = (
        (wld_in, wld), (wqd_in, wqd), (wqu_in, wqu), (wku_in, wku), (wvu_in, wvu), (w_out_in, w_out),
        (tokens_in, normed), (in_gain_in, in_gain), (wrope_in, wrope), (q_lat_gain_in, q_lat_gain),
        (kv_lat_gain_in, kv_lat_gain), (q_gain_in, q_gain), (k_gain_in, k_gain), (table_in, table),
        (out_gain_in, out_gain),
    )
    loads = [pltpu.make_async_copy(src, dst, load_sems.at[n]) for n, (src, dst) in enumerate(pairs)]
    for load in loads:
        load.start()

    def at_sp(target):
        return {"sp": target, "dp": d}

    def at_dp(target):
        return {"sp": s, "dp": target}

    def at_z(target):
        return at_sp(target * ny + y)

    def at_y(step):
        return at_sp(z * ny + lax.rem(y + step, ny))

    def at_x(step):
        return at_dp(lax.rem(x + step, nx) * cores + c)

    def at_core(step):
        return at_dp(x * cores + lax.rem(c + step, cores))

    def back_y(step):
        return lax.rem(y - step + ny, ny)

    def back_x(step):
        return lax.rem(x - step + nx, nx)

    def back_core(step):
        return lax.rem(c - step + cores, cores)

    def near(i):
        m = jnp.minimum(z, nz - 1 - z)
        two = i <= 2 * m
        dist = jnp.where(two, lax.div(i + 1, 2), i - m)
        up = jnp.where(two, lax.rem(i, 2) == 1, z < nz - 1 - z)
        return jnp.where(up, z + dist, z - dist)

    barrier = pltpu.get_barrier_semaphore()
    peers = [at_z(lax.rem(z + k, nz)) for k in range(1, nz)] + [at_y(k) for k in range(1, ny)]
    peers += [at_x(k) for k in range(1, nx)] + [at_core(k) for k in range(1, cores)]
    for peer in peers:
        pl.semaphore_signal(barrier, inc=1, device_id=peer, device_id_type=MESH)
    pl.semaphore_wait(barrier, len(peers))

    for load in loads[:6]:
        load.wait()

    xs, ys, cs, zs = range(1, nx), range(1, ny), range(1, cores), range(1, nzs)

    downs = ((wld, wld_g, DOWN_CUTS[0]), (wqd, wqd_g, DOWN_CUTS[1]))
    items = [(a, cut) for a in range(2) for cut in range(downs[a][2])]

    def piece(ref, a, cut, which):
        cuts = downs[a][2]
        part = ref.shape[0] // (ny * cuts)
        return ref.at[pl.ds(pl.multiple_of((which * cuts + cut) * part, part), part)]

    for it, (a, cut) in enumerate(items):
        src, dst, _ = downs[a]
        for dx in xs:
            links.send(("x", it, dx), piece(src, a, cut, y), piece(dst.at[d], a, cut, y), at_x(dx))
    for a, (src, dst, _) in enumerate(downs):
        for dc in cs:
            links.send(("c", a, dc), src, dst.at[d], at_core(dc))

    ups = ((wqu, wqu_g), (wku, wku_g), (wvu, wvu_g))
    def up_slot(k, dy, dx, cc):
        return lax.rem(zo - k + nzs, nzs), back_y(dy), back_x(dx) * cores + cc

    def up_over_x(a, k, dy, src):
        dst = ups[a][1].at[up_slot(k, dy, 0, c)]
        for dx in xs:
            links.send(("ux", a, k, dy, dx), src, dst, at_x(dx))

    def up_over_y(a, k, src):
        dst = ups[a][1].at[up_slot(k, 0, 0, c)]
        for dy in ys:
            links.send(("uy", a, k, dy), src, dst, at_y(dy))

    def up_over_core(a, k, dy, dx, src):
        dst = ups[a][1].at[up_slot(k, dy, dx, c)]
        for dc in cs:
            links.send(("uc", a, k, dy, dx, dc), src, dst, at_core(dc))

    for a, (src, dst) in enumerate(ups):
        for k in zs:
            links.send(("uz", a, k), src, dst.at[zo, y, d], at_z(lax.rem(z + k * group, nz)))
        up_over_y(a, 0, src)
        up_over_x(a, 0, 0, src)
        up_over_core(a, 0, 0, 0, src)

    def along_z(role, way, origin, src, dst, ok):
        links.send((role, way), src, dst, at_z(jnp.clip(z + way, 0, nz - 1)), ok, at=origin)

    def z_arrival(step, way):
        origin = z - way * (step + 1)
        ok = (origin >= 0) & (origin < nz)
        return jnp.clip(origin, 0, nz - 1), ok, ok & (z + way >= 0) & (z + way < nz)

    def w_over_y(origin, src, ok):
        for dy in ys:
            links.send(("wy", dy), src, w_block(origin, y, x, c), at_y(dy), ok, at=origin)

    def w_over_x(origin, dyo, src, ok):
        for dx in xs:
            links.send(("wx", dyo, dx), src, w_block(origin, back_y(dyo), x, c), at_x(dx), ok, at=origin)

    def w_over_core(origin, dyo, dxo, src, ok):
        for dc in cs:
            dst = w_block(origin, back_y(dyo), back_x(dxo), c)
            links.send(("wc", dyo, dxo, dc), src, dst, at_core(dc), ok, at=origin)

    def w_z_relay(step, onward=True):
        for way in (1, -1):
            origin, ok, more = z_arrival(step, way)
            block = w_block(origin, y, x, c)
            links.arrive(("wz", way), block, at_sp(s), ok, at=origin)
            if onward:
                along_z("wz", way, origin, block, block, more)

    def w_z_onward(step):
        for way in (1, -1):
            origin, ok, more = z_arrival(step, way)
            block = w_block(origin, y, x, c)
            along_z("wz", way, origin, block, block, more)

    def w_z_spread(step):
        for way in (1, -1):
            origin, ok, _ = z_arrival(step, way)
            block = w_block(origin, y, x, c)
            w_over_x(origin, 0, block, ok)
            w_over_core(origin, 0, 0, block, ok)

    def w_y_near(k):
        origin = near(k)
        w_over_y(origin, w_block(origin, y, x, c), None)

    def w_y_copies(origin, turned):
        copies = []
        for dy in ys:
            block = w_block(origin, back_y(dy), x, c)
            if not turned:
                copies += [links.copy(("wx", dy, dx), origin, block, block, at_x(dx)) for dx in xs]
            copies += [links.copy(("wc", dy, 0, dc), origin, block, block, at_core(dc)) for dc in cs]
        return copies

    def w_y_service(origin, turned=False):
        for dy in ys:
            links.arrive(("wy", dy), w_block(origin, back_y(dy), x, c), at_sp(s), at=origin)
        for copy in w_y_copies(origin, turned):
            copy.start()

    def w_x_turn(origin):
        for dx in xs:
            block = w_block(origin, y, back_x(dx), c)
            links.arrive(("wx", 0, dx), block, at_dp(d), at=origin)
            w_over_core(origin, 0, dx, block, None)
            for dy in ys:
                links.send(("wxy", dx, dy), block, block, at_y(dy), at=origin)

    def w_turned(origin):
        for dx in xs:
            for dy in ys:
                block = w_block(origin, back_y(dy), back_x(dx), c)
                links.arrive(("wxy", dx, dy), block, at_dp(d), at=origin)
                w_over_core(origin, dy, dx, block, None)

    def w_x_arrive(origin, dyo):
        for dx in xs:
            block = w_block(origin, back_y(dyo), back_x(dx), c)
            links.arrive(("wx", dyo, dx), block, at_dp(d), at=origin)
            w_over_core(origin, dyo, dx, block, None)

    own_block = w_block(z, y, x, c)
    for way in (1, -1):
        if nz > 1:
            along_z("wz", way, z, w_out, own_block, (z + way >= 0) & (z + way < nz))

    for load in loads[6:]:
        load.wait()

    def norm(i, _):
        step = rows // 4
        band = pl.ds(pl.multiple_of(i * step, step), step)
        normed[band, :] = rms_scale(normed[band, :].astype(jnp.float32), in_gain[...]).astype(jnp.bfloat16)
        return 0

    lax.fori_loop(0, 4, norm, 0)
    rope_key = lax.dot_general(normed[...], wrope[...], NT, preferred_element_type=jnp.float32)
    kv_g[s, rows:, :] = pack_rope(rope_key)

    def down_x(it):
        a, cut = items[it]
        dst = downs[a][1]
        for dx in xs:
            got = piece(dst.at[back_x(dx) * cores + c], a, cut, y)
            links.arrive(("x", it, dx), got, at_dp(d))
            for dy in ys:
                links.send(("y", it, dx, dy), got, got, at_y(dy))
            for dc in cs:
                links.send(("cx", it, dx, dc), got, got, at_core(dc))

    def down_y(it):
        a, cut = items[it]
        dst = downs[a][1]
        for dx in xs:
            for dy in ys:
                got = piece(dst.at[back_x(dx) * cores + c], a, cut, back_y(dy))
                links.arrive(("y", it, dx, dy), got, at_dp(d))
                for dc in cs:
                    links.send(("cy", it, dx, dy, dc), got, got, at_core(dc))

    def settle_down(a):
        dst = downs[a][1]
        for dc in cs:
            links.arrive(("c", a, dc), dst.at[x * cores + back_core(dc)], at_dp(d))
            for it in range(len(items)):
                if items[it][0] != a:
                    continue
                for dx in xs:
                    origin = dst.at[back_x(dx) * cores + back_core(dc)]
                    links.arrive(("cx", it, dx, dc), piece(origin, a, items[it][1], y), at_dp(d))
                    for dy in ys:
                        got = piece(origin, a, items[it][1], back_y(dy))
                        links.arrive(("cy", it, dx, dy, dc), got, at_dp(d))

    def down(gathered):
        part = gathered.shape[1]
        total = None
        for k in range(dps):
            term = jnp.dot(normed[:, k * part : (k + 1) * part], gathered[k], preferred_element_type=jnp.float32)
            total = term if total is None else total + term
        return total

    def kv_over_y(zz, ok=None):
        block = kv_g.at[zz * ny + y]
        for dy in ys:
            links.send(("kvy", dy), block, block, at_y(dy), ok, at=zz)

    def up_arrive(role, a, k, dy, dx):
        got = ups[a][1].at[up_slot(k, dy, dx, c)]
        links.arrive(role, got, at_dp(d))
        return got

    down_x(0)
    down_x(1)
    down_y(0)
    for a in range(3):
        for dy in ys:
            got = up_arrive(("uy", a, 0, dy), a, 0, dy, 0)
            up_over_x(a, 0, dy, got)
            up_over_core(a, 0, dy, 0, got)
    for it in range(2, len(items)):
        down_x(it)
    def up_z(a):
        for k in zs:
            got = up_arrive(("uz", a, k), a, k, 0, 0)
            up_over_y(a, k, got)
            up_over_x(a, k, 0, got)
            up_over_core(a, k, 0, 0, got)

    settle_down(0)
    kv_g[s, :rows, :] = rms_scale(down(wld_g), kv_lat_gain[...]).astype(jnp.bfloat16)
    own_kv = kv_g.at[s]
    along_z("kv", 1, z, own_kv, own_kv, z < nz - 1)
    along_z("kv", -1, z, own_kv, own_kv, z > zb)
    kv_over_y(z)
    for it in range(1, len(items)):
        down_y(it)

    def up_diagonal(a):
        for k in zs:
            for dy in ys:
                got = up_arrive(("uy", a, k, dy), a, k, dy, 0)
                up_over_x(a, k, dy, got)
                up_over_core(a, k, dy, 0, got)

    def up_spread(a, k):
        for dy in range(ny):
            for dx in xs:
                up_over_core(a, k, dy, dx, up_arrive(("ux", a, k, dy, dx), a, k, dy, dx))

    def settle_up(a):
        for k in range(nzs):
            for dy in range(ny):
                for dx in range(nx):
                    for dc in cs:
                        got = ups[a][1].at[up_slot(k, dy, dx, back_core(dc))]
                        links.arrive(("uc", a, k, dy, dx, dc), got, at_dp(d))

    settle_down(1)
    q_g[zl] = rms_scale(down(wqd_g), q_lat_gain[...]).astype(jnp.bfloat16)

    def kv_relay(step):
        for way in (1, -1):
            origin, ok, more = z_arrival(step, way)
            if way < 0:
                base = origin - lax.rem(origin, group)
                ok, more = ok & (z >= base), more & (z - 1 >= base)
            block = kv_g.at[origin * ny + y]
            links.arrive(("kv", way), block, at_sp(s), ok, at=origin)
            along_z("kv", way, origin, block, block, more)
            kv_over_y(origin, ok)

    for a in range(3):
        up_z(a)
    if nz > 1:
        kv_relay(0)
    if nz > 1:
        w_z_relay(0)
    for a in range(3):
        up_diagonal(a)
    for step in range(1, nz - 2):
        kv_relay(step)
    for k in range(1, group):
        links.send(("q", k), q_g.at[zl], q_g.at[zl], at_z(zb + lax.rem(zl + k, group)), at=zl)
    w_over_x(z, 0, w_out, None)
    w_over_core(z, 0, 0, w_out, None)
    if nz > 1:
        w_z_spread(0)
    w_over_y(z, w_out, None)
    for a in range(3):
        up_spread(a, 0)
    for k in zs:
        for a in range(3):
            up_spread(a, k)
    for a in range(3):
        settle_up(a)
    for step in range(1, nz - 2):
        w_z_relay(step)
        w_z_spread(step)
    shards = nzs * ny
    shard_heads = heads // shards
    depth = wqu.shape[0]
    for yy in range(shards):
        for k in range(dps):
            up = wqu_g[yy // ny, yy % ny, k].astype(jnp.float32)
            width = wqu.shape[1] // shard_heads
            for h in range(shard_heads):
                head = up[:, h * width : (h + 1) * width]
                both = jnp.concatenate([head[:, :nope], with_swapped(head[:, nope:])], axis=1)
                wide = both.shape[1]
                first = (yy * shard_heads + h) * wide
                wq_s[k * depth : (k + 1) * depth, first : first + wide] = both.astype(jnp.bfloat16)
        wv = wvu_g[yy // ny, yy % ny].reshape(dps * wvu.shape[0], wvu.shape[1])
        wvt[yy * shard_heads * vd : (yy + 1) * shard_heads * vd, :] = jnp.transpose(
            wv.astype(jnp.float32)
        ).astype(jnp.bfloat16)
    gq, gk = q_gain[:, :nope], k_gain[:, :nope]
    gq2, gk2 = with_swapped(q_gain[:, nope:]), with_swapped(k_gain[:, nope:])
    rope2 = gq2.shape[1]

    def project_kv(block):
        tok = pl.ds(pl.multiple_of(block * rows, rows), rows)
        wks = [wku_g[yy // ny, yy % ny].reshape(dps * wku.shape[0], wku.shape[1]) for yy in range(shards)]
        shared = unpack_rope(kv_g[block, rows:, :], rope2)
        project_keys(block, rows, nope, kv_g[block, :rows, :], shared, wks, wvt, gk, table[tok, :] * gk2, k_s, v_s)

    def kv_column(zz):
        def one(j, _):
            yy = lax.rem(y + j, ny)
            project_kv(zz * ny + yy)
            return 0

        for dy in ys:
            links.arrive(("kvy", dy), kv_g.at[zz * ny + back_y(dy)], at_sp(s), at=zz)
        lax.fori_loop(0, ny, one, 0)

    def kv_columns(first, last):
        def one(i, _):
            inside = zb + lax.rem(zl + i, group)
            kv_column(jnp.where(i < group, inside, zb - 1 - (i - group)))
            return 0

        lax.fori_loop(first, last, one, 0)

    kv_columns(0, 1)
    for step in range(max(nz - 2, 1), nz - 1):
        kv_relay(step)
    for k in range(1, min(2, nz)):
        w_y_near(k)
    for k in range(2, nz - 1):
        w_y_near(k)
    kv_columns(1, zb + group)
    def hand_over(li):
        return links.copy("a2a", li, att_s.at[li], heads_g.at[zl], at_z(zb + li), land=zl)

    def far_w():
        for step in range(max(nz - 2, 1), nz - 1):
            w_z_relay(step, False)
            w_z_spread(step)
        if nz > 2:
            w_y_near(nz - 1)

    def turn_w(k):
        if k < nz:
            if k < TURNED:
                w_x_turn(near(k))
            w_y_service(near(k), k < TURNED)

    def early():
        far_w()
        turn_w(1)

    def late():
        turn_w(2)

    def rest():
        for k in range(3, nz):
            turn_w(k)

    def attend(i, between):
        li = lax.rem(zl + 1 + i, group)
        for k in range(1, group):
            links.arrive(("q", k), q_g.at[li], at_sp(s), li == lax.rem(zl - k + group, group), at=li)
        zz = zb + li
        qb = zz * ny + y
        tok = pl.ds(pl.multiple_of(qb * rows, rows), rows)
        project_queries(rows, heads, nope, q_g[li], wq_s, gq, table[tok, :] * gq2, q_s)
        att_s[li] = attend_block(
            zz, y, rows, chunk, heads, vd, scale, q_s, k_s, v_s, m_s, l_s, work, between
        )
        if i < group - 1:
            hand_over(li).start()

    turn_w(0)
    for i in range(group):
        attend(i, early if i == 0 else late if i == 1 else lambda: None)
    if group < 2:
        late()
    rest()
    heads_g[zl] = att_s[zl]
    for k in range(1, group):
        li = lax.rem(zl + k, group)
        hand_over(li).wait_send()
        links.copy("a2a", li, heads_g.at[li], heads_g.at[li], at_z(zb + li), land=li).wait_recv()
    width = heads * vd
    band = width // nzs
    square = jnp.zeros((rows, 1), jnp.float32)
    for k in range(group):
        block = heads_g[k].astype(jnp.float32)
        square = square + jnp.sum(block * block, axis=-1, keepdims=True)
    r = lax.rsqrt(square * (1.0 / (group * width)) + EPS)
    for k in range(group):
        for j in range(nzs):
            cols = slice((j * group + k) * band, (j * group + k + 1) * band)
            part = heads_g[k, :, j * band : (j + 1) * band].astype(jnp.float32)
            normed[:, cols] = (part * r * out_gain[:, cols]).astype(jnp.bfloat16)
    for k in range(nz):
        if k >= TURNED:
            w_x_arrive(near(k), 0)

    def settle_w(origin, dy):
        for dx in range(nx):
            for dc in cs:
                block = w_block(origin, back_y(dy), back_x(dx), back_core(dc))
                links.arrive(("wc", dy, dx, dc), block, at_dp(d), at=origin)

    for k in range(nz):
        settle_w(near(k), 0)
    tile = rows * max(1, 512 // rows)
    run = dps * part_out

    def add_out(blocks, first, last):
        def one(i, _):
            at = pl.multiple_of(i * tile, tile)
            cols = pl.ds(at, tile)
            held = [work.at[pl.ds(pl.multiple_of(at + j * rows, rows), rows)] for j in range(tile // rows)]
            total = None if first else jnp.concatenate([h[...] for h in held], axis=1)
            for zz, yy in blocks:
                at_rows = pl.ds(pl.multiple_of((zz * ny + yy) * run, run), run)
                term = jnp.dot(normed[:, at_rows], w_g[at_rows, cols], preferred_element_type=jnp.float32)
                total = term if total is None else total + term
            if last:
                out[:, cols] = total.astype(out.dtype)
            else:
                for j in range(tile // rows):
                    held[j][...] = total[:, j * rows : (j + 1) * rows]
            return 0

        lax.fori_loop(0, out.shape[1] // tile, one, 0)

    def finish_w(k):
        if k < TURNED:
            w_turned(near(k))
        else:
            for dy in ys:
                w_x_arrive(near(k), dy)

    add_out([(near(k), y) for k in range(nz)], True, ny == 1)
    others = [[(near(k), back_y(dy)) for dy in ys] for k in range(nz)]
    phases = ([k for k in range(nz - 1)], [nz - 1]) if nz > 1 else ([0],)
    for phase in phases if ny > 1 else ():
        for k in phase:
            finish_w(k)
        for k in phase:
            for dy in ys:
                settle_w(near(k), dy)
        add_out(sum([others[k] for k in phase], []), False, phase is phases[-1])
    for k in range(nz):
        for copy in w_y_copies(near(k), k < TURNED):
            copy.wait_send()
    links.drain()


def per_device(
    tokens, in_gain, w_query_down, w_latent_down, w_rope_key, query_latent_gain, latent_gain,
    w_query_up, w_key_up, w_value_up, query_gain, key_gain, out_gain, w_out,
):
    seqs, dps = lax.axis_size("sp"), lax.axis_size("dp")
    cores = 2 if dps % 2 == 0 else 1
    nx = dps // cores
    ny = nx if seqs % nx == 0 else 1
    nz = seqs // ny
    group = 2 if nz % 2 == 0 else nz
    heads = HEADS // group
    shards = seqs // group
    own_rows = tokens.shape[1]
    length = own_rows * seqs
    rope = w_rope_key.shape[1]
    nope = w_key_up.shape[1] * shards // heads
    vd = w_value_up.shape[1] * shards // heads
    wide = nope + 2 * rope
    chunk = ny * own_rows
    sems, sem_rows = sem_counts(nx, ny, nz, cores, group)
    b16 = jnp.bfloat16

    def gathered(w, *lead):
        return pltpu.VMEM(lead + (dps,) + w.shape, b16)

    result = pl.pallas_call(
        functools.partial(
            layer_kernel, (nx, ny, nz, cores, group), chunk, heads, nope, vd, float(nope + rope) ** -0.5
        ),
        out_shape=pltpu.VMEM((own_rows, w_out.shape[1]), b16),
        in_specs=[pl.BlockSpec(memory_space=pltpu.HBM)] * 15,
        out_specs=pl.BlockSpec(memory_space=pltpu.VMEM),
        scratch_shapes=[
            pltpu.VMEM((1, tokens.shape[2]), jnp.float32),
            pltpu.VMEM((rope, tokens.shape[2]), b16),
            pltpu.VMEM((1, w_query_down.shape[1]), jnp.float32),
            pltpu.VMEM((1, w_latent_down.shape[1]), jnp.float32),
            pltpu.VMEM((1, nope + rope), jnp.float32),
            pltpu.VMEM((1, nope + rope), jnp.float32),
            pltpu.VMEM((length, 2 * rope), jnp.float32),
            pltpu.VMEM((1, out_gain.shape[0]), jnp.float32),
            pltpu.VMEM((own_rows, tokens.shape[2]), b16),
            gathered(w_query_down), gathered(w_latent_down),
            gathered(w_query_up, nz // group, ny), gathered(w_key_up, nz // group, ny), gathered(w_value_up, nz // group, ny),
            pltpu.VMEM((w_out.shape[0] * seqs * dps, w_out.shape[1]), b16),
            pltpu.VMEM((w_query_down.shape[1], heads * wide), b16),
            pltpu.VMEM((heads * vd, w_latent_down.shape[1]), b16),
            pltpu.VMEM((seqs, own_rows + own_rows * rope // w_latent_down.shape[1], w_latent_down.shape[1]), b16),
            pltpu.VMEM((group, own_rows, w_query_down.shape[1]), b16),
            pltpu.VMEM((heads, own_rows, wide), b16),
            pltpu.VMEM((heads, length, wide), b16),
            pltpu.VMEM((heads * vd, length), b16),
            pltpu.VMEM((heads, 1, own_rows), jnp.float32),
            pltpu.VMEM((heads, 1, own_rows), jnp.float32),
            pltpu.VMEM((max(heads * vd + 2 * chunk, w_out.shape[1]), own_rows), jnp.float32),
            pltpu.VMEM((group, own_rows, heads * vd), b16),
            pltpu.VMEM((group, own_rows, heads * vd), b16),
            pltpu.SemaphoreType.DMA((sems,)),
            pltpu.SemaphoreType.DMA((sems,)),
            pltpu.SemaphoreType.DMA((sem_rows, nz)),
            pltpu.SemaphoreType.DMA((sem_rows, nz)),
            pltpu.SemaphoreType.DMA((15,)),
        ],
        compiler_params=pltpu.CompilerParams(
            vmem_limit_bytes=min(62, 56 * length // 2048) * 1024 * 1024, collective_id=0, has_side_effects=True
        ),
        cost_estimate=pl.CostEstimate(flops=60 * 10**9, bytes_accessed=10**8, transcendentals=5 * 10**6),
    )(
        tokens.reshape(own_rows, tokens.shape[2]), in_gain[None], w_query_down, w_latent_down, w_rope_key.T,
        query_latent_gain[None], latent_gain[None], w_query_up, w_key_up, w_value_up,
        query_gain[None], key_gain[None], jnp.asarray(rotation_table(length, rope)), out_gain[None], w_out,
    )
    return result.reshape(1, own_rows, w_out.shape[1])


def solution(mesh):
    in_specs = (
        P("dp", "sp", None), P(), P("dp", None), P("dp", None), P(), P(), P(),
        P("dp", "sp"), P("dp", "sp"), P("dp", "sp"), P(), P(), P(), P(("sp", "dp"), None),
    )
    return jax.shard_map(
        per_device, mesh=mesh, in_specs=in_specs, out_specs=P("dp", "sp", None), check_vma=False
    )
```
